32 devices in a mesh: grp: 2 (over x), row: 4 (over z), col: 4 (over y, core).
Axes of the slice: x: 2, y: 2, z: 4, core: 2. Of those that a mesh axis runs over, the one named last changes fastest.
Arguments:
- tokens: bfloat16 [2, 2048, 2048], P('grp', ('row', 'col')), parts along dimension 0, may hold values from -6 to 6
- norm_gain: bfloat16 [2048], replicated, may hold values from 0.099609375 to 1.8984375
- w_in: bfloat16 [2048, 512], replicated, may hold values from -0.125 to 0.125
- w_out: bfloat16 [512, 2048], replicated, may hold values from -0.25 to 0.25
Outputs:
- mixed: bfloat16 [2, 2048, 2048], P('grp', ('row', 'col')), parts along dimension 0
The draws below stay inside these ranges and needn't reach their ends.
There are 2 independent parts, one for each index of `grp`. The reference program is written for one: setup_inputs(seed, part) draws one part's arguments, and reference() takes and returns one part's arrays. A program takes and returns all parts, laid end to end along the dimension named above; an argument that names none is the same for every part. Nothing has to cross between parts.
All inputs are finite; a program needn't handle non-finite values.
Results may differ from the reference program's by a relative error of at most 0.013.
Values may be sent and summed in bfloat16 or wider, within the bound.
A program may use at most 64 MiB of HBM per device.

```python
import jax
import jax.numpy as jnp
from jax import lax

D = 2048
FEATS = 512
GROUP_CH = 128
SEQS = 1
LENGTH = 2048


def level_of(rng, dims, pieces, low, high):
    factor_of = 1.0
    for dim, shards_of in pieces:
        steps = jax.random.uniform(jax.random.fold_in(jax.random.fold_in(rng, 6), dim), (shards_of,), jnp.float32, low / len(pieces), high / len(pieces))
        factor_of = factor_of * jnp.repeat(jnp.exp(steps), dims[dim] // shards_of).reshape((-1,) + (1,) * (len(dims) - 1 - dim))
    return factor_of


def bell_draw(key, shape, spread, bound, split=(), held_as=jnp.bfloat16):
    factor_of = level_of(key, shape, split, -0.22, 0.18) if split else 1.0
    result = jax.random.normal(key, shape, jnp.float32) * spread * factor_of
    return jnp.minimum(jnp.maximum(result, -bound), bound).astype(held_as)


def setup_inputs(seed: int = 0, part: int = 0) -> dict:
    key_of = jax.random.split(jax.random.key(seed), 5)
    part_splits = jax.random.split(jax.random.fold_in(key_of[4], part), 5)
    tokens = bell_draw(part_splits[0], (SEQS, LENGTH, D), 1.0, 6.0, ((1, 16),))
    norm_gain = jnp.clip(1.0 + 0.18 * jax.random.normal(key_of[1], (D,), jnp.float32), 0.099609375, 1.8984375).astype(jnp.bfloat16)
    w_in = bell_draw(key_of[2], (D, FEATS), D ** -0.5, 0.125)
    w_out = bell_draw(key_of[3], (FEATS, D), FEATS ** -0.5, 0.25)
    return {"tokens": tokens, "norm_gain": norm_gain, "w_in": w_in, "w_out": w_out}


def reference(tokens, norm_gain, w_in, w_out):
    widened = tokens.astype(jnp.float32)
    factor = lax.rsqrt(lax.optimization_barrier(jnp.mean(widened * widened, -1, keepdims=True)) + 1e-06)
    normed = (widened * factor * norm_gain.astype(jnp.float32)).astype(jnp.bfloat16)
    flat = normed.reshape(SEQS * LENGTH, D)
    mixin = jnp.dot(flat, w_in, preferred_element_type=jnp.float32).astype(jnp.bfloat16)
    grouped = mixin.astype(jnp.float32).reshape(SEQS, LENGTH, FEATS // GROUP_CH, GROUP_CH)
    spectrum = jnp.fft.fft2(grouped, axes=(1, 3), norm='ortho').real
    spectrum = spectrum.astype(jnp.float32).reshape(SEQS * LENGTH, FEATS).astype(jnp.bfloat16)
    mixed = jnp.dot(spectrum, w_out, preferred_element_type=jnp.float32).astype(jnp.bfloat16)
    return mixed.reshape(SEQS, LENGTH, D)
```

```python
import functools
import math

import jax
import jax.numpy as jnp
import numpy as np
from jax import lax
from jax.experimental import pallas as pl
from jax.experimental.pallas import tpu as pltpu
from jax.sharding import PartitionSpec as P

GROUP_CH = 128


TWO_PI = 2.0 * math.pi
NORM_EPS = 1e-06
HIGHEST = lax.Precision.HIGHEST


def phase_tables(rows, cols, period):
    left = lax.broadcasted_iota(jnp.int32, (rows, cols), 0)
    right = lax.broadcasted_iota(jnp.int32, (rows, cols), 1)
    angles = (left * right % period).astype(jnp.float32) * (TWO_PI / period)
    return (jnp.cos(angles), jnp.sin(angles))


def rotate_by(pattern, cos_table, sin_table, real_part, imag_part):

    def apply(table, data):
        return jnp.einsum(pattern, table, data, precision=HIGHEST)

    return (
        apply(cos_table, real_part) + apply(sin_table, imag_part),
        apply(cos_table, imag_part) - apply(sin_table, real_part),
    )


def twist(real_part, imag_part, cos_table, sin_table):
    return (
        real_part * cos_table + imag_part * sin_table,
        imag_part * cos_table - real_part * sin_table,
    )


def factored_shards(tokens, norm_gain, w_in, w_out):
    seq_count, tok_count, width = tokens.shape
    feat_count = w_in.shape[1]
    row_count = lax.axis_size("row")
    col_count = lax.axis_size("col")
    block_len = tok_count * col_count
    length = block_len * row_count
    sub_feats = feat_count // row_count
    fine_count = tok_count // row_count
    item_count = seq_count * feat_count // col_count
    ortho_scale = 1.0 / math.sqrt(length * GROUP_CH)
    widened = tokens.astype(jnp.float32)
    factor = lax.rsqrt(jnp.mean(widened * widened, -1, keepdims=True) + NORM_EPS)
    normed = (widened * factor * norm_gain.astype(jnp.float32)).astype(jnp.bfloat16)
    mixin = jnp.einsum("std,df->sft", normed, w_in, preferred_element_type=jnp.float32).astype(
        jnp.bfloat16
    )
    row_cos, row_sin = phase_tables(row_count, row_count, row_count)
    chan_cos, chan_sin = phase_tables(GROUP_CH, GROUP_CH, GROUP_CH)
    stacked_shape = (seq_count, sub_feats, row_count, tok_count)
    grouped = mixin.astype(jnp.float32).reshape(
        seq_count, feat_count // GROUP_CH, GROUP_CH, tok_count
    )
    spec_real = jnp.einsum("sgqt,qm->sgmt", grouped, chan_cos, precision=HIGHEST).reshape(
        seq_count, feat_count, tok_count
    )
    spec_imag = -jnp.einsum("sgqt,qm->sgmt", grouped, chan_sin, precision=HIGHEST).reshape(
        seq_count, feat_count, tok_count
    )
    arrived = (
        lax.all_to_all(
            spec_real.astype(jnp.bfloat16), "row", split_axis=1, concat_axis=2, tiled=True
        ).astype(spec_real.dtype),
        lax.all_to_all(
            spec_imag.astype(jnp.bfloat16), "row", split_axis=1, concat_axis=2, tiled=True
        ).astype(spec_imag.dtype),
    )
    stacked_real = arrived[0].reshape(stacked_shape)
    stacked_imag = arrived[1].reshape(stacked_shape)
    real_part, imag_part = rotate_by("ka,sfat->skft", row_cos, row_sin, stacked_real, stacked_imag)
    freq_low = lax.broadcasted_iota(jnp.int32, (row_count, tok_count), 0)
    place = lax.axis_index("col") * tok_count + lax.broadcasted_iota(
        jnp.int32, (row_count, tok_count), 1
    )
    angles = (freq_low * place % length).astype(jnp.float32) * (TWO_PI / length)
    real_part, imag_part = twist(
        real_part, imag_part, jnp.cos(angles)[None, :, None, :], jnp.sin(angles)[None, :, None, :]
    )
    sending = (
        real_part.reshape(item_count, col_count, 1, tok_count),
        imag_part.reshape(item_count, col_count, 1, tok_count),
    )
    col_cos, col_sin = phase_tables(col_count, col_count, col_count)
    mid_cos, mid_sin = phase_tables(col_count, tok_count, block_len)
    tok_cos, tok_sin = phase_tables(tok_count, tok_count, tok_count)
    tok_cos = tok_cos.reshape(row_count, fine_count, tok_count)
    tok_sin = tok_sin.reshape(row_count, fine_count, tok_count)
    span_real, span_imag = rotate_by(
        "uc,qct->qut",
        col_cos,
        col_sin,
        lax.all_to_all(
            sending[0].astype(jnp.bfloat16), "col", split_axis=1, concat_axis=2, tiled=True
        ).astype(jnp.float32)[:, 0],
        lax.all_to_all(
            sending[1].astype(jnp.bfloat16), "col", split_axis=1, concat_axis=2, tiled=True
        ).astype(jnp.float32)[:, 0],
    )
    span_real, span_imag = twist(span_real, span_imag, mid_cos, mid_sin)
    span_real, span_imag = rotate_by("rjt,qut->rjuq", tok_cos, tok_sin, span_real, span_imag)
    owner_shape = (row_count, col_count, fine_count, span_real.shape[-1], 1)
    span_real, span_imag = (span_real.reshape(owner_shape), span_imag.reshape(owner_shape))
    rounded = (span_real * ortho_scale).astype(jnp.bfloat16)
    returned = lax.all_to_all(rounded, "col", split_axis=1, concat_axis=4, tiled=True)
    layout = (row_count, fine_count, seq_count, row_count, sub_feats)
    spectrum = lax.all_to_all(
        returned.reshape(layout), "row", split_axis=0, concat_axis=4, tiled=True
    )
    spectrum = spectrum.reshape(fine_count, seq_count, row_count, feat_count)
    mixed = jnp.einsum("jskf,fd->sjkd", spectrum, w_out, preferred_element_type=jnp.float32).astype(
        jnp.bfloat16
    )
    return mixed.reshape(seq_count, fine_count * row_count, width)


LANES = 128
SUBLANES = 8
CHUNKS = 2
PIECES = 4
MESH = pl.DeviceIdType.MESH
NT = (((1,), (1,)), ((), ()))


def fused_fits(row_count, peers, tok_count, feat_count):
    if row_count % (2 * CHUNKS) or feat_count % (GROUP_CH * CHUNKS):
        return False
    if feat_count % peers or tok_count % peers or GROUP_CH != LANES:
        return False
    slots = feat_count // peers
    return (
        tok_count == LANES
        and slots % (4 * SUBLANES) == 0
        and LANES % slots == 0
        and peers % (LANES // slots) == 0
        and feat_count % GROUP_CH == 0
        and (tok_count // peers) % SUBLANES == 0
    )


def host_tables(peers, tok_count, feat_count):
    length = peers * tok_count
    slots = feat_count // peers
    half = slots // 2
    per_lane = LANES // slots
    stacks = peers // per_lane
    fine = tok_count // peers
    members = GROUP_CH // slots
    chan = np.zeros((GROUP_CH, GROUP_CH))
    chan_at = np.zeros((GROUP_CH,), np.int64)
    q = np.arange(GROUP_CH)
    for m in range(GROUP_CH // 2):
        row = m // half * slots + m % half
        chan[row] = np.cos(2 * np.pi * (q * m % GROUP_CH) / GROUP_CH)
        chan_at[row] = m
        if m:
            chan[row + half] = -np.sin(2 * np.pi * (q * m % GROUP_CH) / GROUP_CH)
            chan_at[row + half] = GROUP_CH - m
        else:
            chan[row + half] = np.cos(np.pi * q)
            chan_at[row + half] = GROUP_CH // 2
    t = np.arange(tok_count)
    b = np.arange(tok_count)[:, None]
    scale = 1.0 / math.sqrt(length * GROUP_CH)
    mid = np.zeros((stacks, tok_count, per_lane, 2, tok_count))
    for g in range(stacks):
        for a in range(per_lane):
            k = peers * b + g * per_lane + a
            angle = 2 * np.pi * (t * k % length) / length
            mid[g, :, a, 0] = np.cos(angle) * scale
            mid[g, :, a, 1] = np.sin(angle) * scale
    mid = mid.reshape(stacks, tok_count, per_lane * 2 * tok_count)
    pick = np.zeros((members, per_lane, slots, per_lane, GROUP_CH))
    for dd in range(members):
        for a in range(per_lane):
            for c in range(slots):
                pick[dd, a, c, a, chan_at[dd * slots + c]] = 1
    pick = pick.reshape(members * LANES, per_lane * GROUP_CH)
    return [jnp.asarray(x, jnp.bfloat16) for x in (chan, mid, pick)]


def short_transform(blocks):
    n = len(blocks)
    even = [blocks[0]] + [blocks[s] + blocks[n - s] for s in range(1, n // 2)] + [blocks[n // 2]]
    odd = [None] + [blocks[s] - blocks[n - s] for s in range(1, n // 2)]

    def combine(terms):
        groups = {}
        for coef, term in terms:
            if abs(coef) < 1e-9:
                continue
            size = round(abs(coef), 9)
            signed = groups.get(size)
            if signed is None:
                groups[size] = term if coef > 0 else -term
            else:
                groups[size] = signed + term if coef > 0 else signed - term
        total = None
        for size, value in groups.items():
            value = value if size == 1.0 else value * size
            total = value if total is None else total + value
        return total

    out = []
    for a in range(n // 2 + 1):
        cos_part = combine(
            [(math.cos(TWO_PI * (s * a % n) / n), even[s]) for s in range(n // 2 + 1)]
        )
        sin_part = combine([(math.sin(TWO_PI * (s * a % n) / n), odd[s]) for s in range(1, n // 2)])
        if sin_part is None:
            sin_part = jnp.zeros_like(cos_part)
        out.append((cos_part, sin_part))
    for a in range(n // 2 + 1, n):
        out.append((out[n - a][0], -out[n - a][1]))
    return out


def fused_kernel(
    shape,
    chunks,
    tokens_hbm,
    gain_hbm,
    w_in_hbm,
    chan_hbm,
    mid_hbm,
    pick_hbm,
    w_out_hbm,
    last_ref,
    partial_ref,
    w_last,
    tokens,
    gain,
    w_in,
    chan,
    mid,
    pick,
    w_first,
    natural,
    first_out,
    first_in,
    blocks,
    second_out,
    second_in,
    load_sem,
    send_a,
    recv_a,
    send_b,
    recv_b,
):
    row_count, col_count = shape
    peers = row_count * col_count
    tok_count, width = tokens.shape
    feat_count = w_in.shape[1]
    slots = feat_count // peers
    half = slots // 2
    per_lane = LANES // slots
    stacks = peers // per_lane
    fine = tok_count // peers
    members = GROUP_CH // slots
    groups = feat_count // GROUP_CH
    hosts = peers // chunks
    host_rows = row_count // chunks
    low_row = (row_count - host_rows) // 2
    high_row = low_row + host_rows - 1
    part_groups = groups // chunks
    part_feats = feat_count // chunks
    row, col = lax.axis_index("row"), lax.axis_index("col")
    me = row * col_count + col
    is_host = (row >= low_row) & (row <= high_row)
    host = jnp.where(is_host, me - low_row * col_count, 0)

    def device(index):
        return {"row": index // col_count, "col": lax.rem(index, col_count)}

    depth = width // PIECES
    load_tokens = pltpu.make_async_copy(tokens_hbm, tokens, load_sem.at[0])
    load_gain = pltpu.make_async_copy(gain_hbm, gain, load_sem.at[1])
    load_chan = pltpu.make_async_copy(chan_hbm, chan, load_sem.at[2])
    load_mid = pltpu.make_async_copy(mid_hbm, mid, load_sem.at[3])
    load_pick = pltpu.make_async_copy(pick_hbm, pick, load_sem.at[4])
    first_feats = feat_count - part_feats
    load_first = pltpu.make_async_copy(
        w_out_hbm.at[pl.ds(0, first_feats)], w_first, load_sem.at[5]
    )
    load_last = pltpu.make_async_copy(
        w_out_hbm.at[pl.ds(first_feats, part_feats)], w_last, load_sem.at[6]
    )
    load_w = []
    for c in range(chunks):
        for i in range(PIECES):
            at = (pl.ds(i * depth, depth), pl.ds(c * part_feats, part_feats))
            load_w.append(
                pltpu.make_async_copy(
                    w_in_hbm.at[at], w_in.at[at], load_sem.at[7 + c * PIECES + i]
                )
            )
    load_tokens.start()
    load_gain.start()
    for load in load_w[:PIECES]:
        load.start()
    load_chan.start()
    for load in load_w[PIECES:]:
        load.start()

    barrier = pltpu.get_barrier_semaphore()

    @pl.when(is_host)
    def _():
        for step in range(1, peers):
            target = lax.rem(me + step, peers)
            pl.semaphore_signal(barrier, inc=1, device_id=device(target), device_id_type=MESH)

    host_order = []
    for i in range(host_rows):
        target_row = jnp.where(row * 2 < row_count, high_row - i, low_row + i)
        host_order += [
            (target_row * col_count + lax.rem(col + shift, col_count), shift == 0)
            for shift in [*range(1, col_count), 0]
        ]

    def first_copy(c, target):
        spot = c * hosts + target - low_row * col_count
        return pltpu.make_async_remote_copy(
            src_ref=first_out.at[spot],
            dst_ref=first_in.at[c, me],
            send_sem=send_a.at[spot],
            recv_sem=recv_a.at[c, me],
            device_id=device(target),
            device_id_type=MESH,
        )

    def each_host(c, act):
        for target, may_be_me in host_order:
            if may_be_me:

                @pl.when(target != me)
                def _():
                    act(first_copy(c, target))
            else:
                act(first_copy(c, target))

    load_tokens.wait()
    load_gain.wait()
    scaled = tokens[...] * gain[...].reshape(1, width)
    widened = tokens[...].astype(jnp.float32)
    factor = lax.rsqrt(jnp.mean(widened * widened, -1, keepdims=True) + NORM_EPS)
    for c in range(chunks):
        mixin = None
        for i in range(PIECES):
            load_w[c * PIECES + i].wait()
            term = jnp.dot(
                scaled[:, i * depth : (i + 1) * depth],
                w_in[i * depth : (i + 1) * depth, c * part_feats : (c + 1) * part_feats],
                preferred_element_type=jnp.float32,
            )
            mixin = term if mixin is None else mixin + term
        mixin = (mixin * factor).astype(jnp.bfloat16)
        if c == 0:
            load_chan.wait()
        if c == chunks - 1:

            @pl.when(is_host)
            def _():
                load_mid.start()

            load_pick.start()
            load_first.start()
            load_last.start()
        for g in range(part_groups):
            spec = lax.dot_general(
                chan[...],
                mixin[:, g * GROUP_CH : (g + 1) * GROUP_CH],
                NT,
                preferred_element_type=jnp.float32,
            ).astype(jnp.bfloat16)
            for dd in range(members):
                spot = (c * part_groups + g) * members + dd
                first_out[spot] = spec[dd * slots : (dd + 1) * slots]
        if c == 0:

            @pl.when(is_host)
            def _():
                pl.semaphore_wait(barrier, hosts - 1)

            @pl.when(jnp.logical_not(is_host))
            def _():
                pl.semaphore_wait(barrier, hosts)

        each_host(c, lambda copy: copy.start())

    def landing(spot):
        lanes = pl.ds(pl.multiple_of(lax.rem(spot, members) * LANES, LANES), LANES)
        return second_in.at[spot // members, :, lanes]

    def second_copy(c, target):
        spot = c * hosts + host
        return pltpu.make_async_remote_copy(
            src_ref=second_out.at[c, target],
            dst_ref=landing(spot),
            send_sem=send_b.at[c, target],
            recv_sem=recv_b.at[spot],
            device_id=device(target),
            device_id_type=MESH,
        )

    @pl.when(is_host)
    def _():
        blocks[...] = jnp.zeros_like(blocks)
        for c in range(chunks):
            first_in[c, me] = first_out[c * hosts + host]
        load_mid.wait()
        for c in range(chunks):
            spot = c * hosts + host
            for step in range(1, peers):
                source = lax.rem(me + step, peers)
                pltpu.make_async_copy(
                    first_in.at[c, source], first_in.at[c, source], recv_a.at[c, source]
                ).wait()
            arrived = [first_in[c, s].astype(jnp.float32) for s in range(peers)]
            place = lax.broadcasted_iota(jnp.int32, (half, tok_count), 0) + spot * half
            paired = lax.rem(place, GROUP_CH // 2) != 0
            spectra = short_transform(arrived)
            for a, (cos_part, sin_part) in enumerate(spectra):
                a_cos, b_cos = cos_part[:half], cos_part[half:]
                a_sin, b_sin = sin_part[:half], sin_part[half:]
                at = a % per_lane
                left = at * 2 * tok_count
                tops = slice(at * slots, at * slots + half)
                lows = slice(at * slots + half, (at + 1) * slots)
                cosines = slice(left, left + tok_count)
                sines = slice(left + tok_count, left + 2 * tok_count)
                g = a // per_lane
                blocks[c, g, tops, cosines] = jnp.where(paired, a_cos + b_sin, a_cos).astype(
                    jnp.bfloat16
                )
                blocks[c, g, tops, sines] = jnp.where(paired, b_cos - a_sin, -a_sin).astype(
                    jnp.bfloat16
                )
                blocks[c, g, lows, cosines] = jnp.where(paired, a_cos - b_sin, b_cos).astype(
                    jnp.bfloat16
                )
                blocks[c, g, lows, sines] = jnp.where(paired, -a_sin - b_cos, -b_sin).astype(
                    jnp.bfloat16
                )
            found = []
            for g in range(stacks):
                value = lax.dot_general(mid[g], blocks[c, g], NT, preferred_element_type=jnp.float32)
                found.append(value.reshape(peers, fine, LANES))
            second_out[c] = jnp.concatenate(found, axis=1).astype(jnp.bfloat16)
            edge_rows = []
            for i in range(low_row):
                edge_rows += [i, row_count - 1 - i]
            for edge in edge_rows:
                for target in range(edge * col_count, (edge + 1) * col_count):
                    second_copy(c, target).start()
            for i in range(1, host_rows + 1):
                target_row = low_row + lax.rem(row - low_row + i, host_rows)
                for shift in range(1 if i == host_rows else 0, col_count):
                    target = target_row * col_count + lax.rem(col + shift, col_count)
                    second_copy(c, target).start()
            landing(spot)[...] = second_out[c, me]

    for c in range(chunks):
        each_host(c, lambda copy: copy.wait_send())

    load_pick.wait()
    load_first.wait()
    for c in range(chunks):

        def arrival(spot):
            pltpu.make_async_copy(landing(spot), landing(spot), recv_b.at[spot]).wait()

        for step in range(1, hosts):
            arrival(c * hosts + lax.rem(host + step, hosts))

        @pl.when(jnp.logical_not(is_host))
        def _():
            arrival(c * hosts + host)

        flat = second_in[c * part_groups : (c + 1) * part_groups].reshape(
            part_groups * stacks * fine, members * LANES
        )
        picked = jnp.dot(flat, pick[...], preferred_element_type=jnp.float32)
        for group in range(part_groups):
            slab = c * part_groups + group
            for g in range(stacks):
                top = (group * stacks + g) * fine
                for a in range(per_lane):
                    natural[slab, pl.ds(g * per_lane + a, fine, stride=peers), :] = picked[
                        top : top + fine, a * GROUP_CH : (a + 1) * GROUP_CH
                    ]
        if c < chunks - 1:
            term = None
            for group in range(part_groups):
                slab = c * part_groups + group
                part = jnp.dot(
                    natural[slab].astype(jnp.bfloat16),
                    w_first[slab * GROUP_CH : (slab + 1) * GROUP_CH, :],
                    preferred_element_type=jnp.float32,
                )
                term = part if term is None else term + part
            if c == 0:
                partial_ref[...] = term
            else:
                partial_ref[...] += term
        if c == chunks - 2:

            @pl.when(is_host)
            def _():
                for each in range(chunks):
                    for step in range(1, peers):
                        second_copy(each, lax.rem(me + step, peers)).wait_send()

            load_last.wait()
        if c == chunks - 1:
            for group in range(part_groups):
                last_ref[:, group * GROUP_CH : (group + 1) * GROUP_CH] = natural[
                    c * part_groups + group
                ].astype(last_ref.dtype)


def project_kernel(chunks, last, partial, w_last, out_hbm, staged, sems):
    size = w_last.shape[1] // chunks
    copies = []
    for i in range(chunks):
        lanes = slice(i * size, (i + 1) * size)
        staged[:, lanes] = (
            partial[:, lanes]
            + jnp.dot(last[...], w_last[:, lanes], preferred_element_type=jnp.float32)
        ).astype(staged.dtype)
        span = pl.ds(i * size, size)
        copy = pltpu.make_async_copy(staged.at[:, span], out_hbm.at[:, span], sems.at[i])
        copy.start()
        copies.append(copy)
    for copy in copies:
        copy.wait()


def fused_shards(tokens, norm_gain, w_in, w_out):
    seq_count, tok_count, width = tokens.shape
    feat_count = w_in.shape[1]
    shape = (lax.axis_size("row"), lax.axis_size("col"))
    peers = shape[0] * shape[1]
    slots = feat_count // peers
    per_lane = LANES // slots
    stacks = peers // per_lane
    fine = tok_count // peers
    members = GROUP_CH // slots
    groups = feat_count // GROUP_CH
    part_feats = feat_count // CHUNKS
    tables = host_tables(peers, tok_count, feat_count)
    operands = [tokens.reshape(tok_count, width), norm_gain, w_in, *tables]
    held = [pltpu.VMEM(x.shape, x.dtype) for x in operands]
    last, partial, w_last = pl.pallas_call(
        functools.partial(fused_kernel, shape, CHUNKS),
        out_shape=(
            pltpu.VMEM((tok_count, part_feats), jnp.bfloat16),
            pltpu.VMEM((tok_count, width), jnp.float32),
            pltpu.VMEM((part_feats, width), jnp.bfloat16),
        ),
        in_specs=[pl.BlockSpec(memory_space=pltpu.HBM)] * (len(operands) + 1),
        out_specs=(pl.BlockSpec(memory_space=pltpu.VMEM),) * 3,
        scratch_shapes=held
        + [
            pltpu.VMEM((feat_count - part_feats, width), jnp.bfloat16),
            pltpu.VMEM((groups, tok_count, GROUP_CH), jnp.float32),
            pltpu.VMEM((peers, slots, tok_count), jnp.bfloat16),
            pltpu.VMEM((CHUNKS, peers, slots, tok_count), jnp.bfloat16),
            pltpu.VMEM((CHUNKS, stacks, LANES, per_lane * 2 * tok_count), jnp.bfloat16),
            pltpu.VMEM((CHUNKS, peers, stacks * fine, LANES), jnp.bfloat16),
            pltpu.VMEM((peers // members, stacks * fine, members * LANES), jnp.bfloat16),
            pltpu.SemaphoreType.DMA((7 + CHUNKS * PIECES,)),
            pltpu.SemaphoreType.DMA((peers,)),
            pltpu.SemaphoreType.DMA((CHUNKS, peers)),
            pltpu.SemaphoreType.DMA((CHUNKS, peers)),
            pltpu.SemaphoreType.DMA((peers,)),
        ],
        compiler_params=pltpu.CompilerParams(
            collective_id=0, has_side_effects=True, vmem_limit_bytes=62_000_000
        ),
    )(*operands, w_out)
    pieces = max(1, width // 512)
    mixed = pl.pallas_call(
        functools.partial(project_kernel, pieces),
        out_shape=jax.ShapeDtypeStruct((tok_count, width), jnp.bfloat16),
        in_specs=[pl.BlockSpec(memory_space=pltpu.VMEM)] * 3,
        out_specs=pl.BlockSpec(memory_space=pltpu.HBM),
        scratch_shapes=[
            pltpu.VMEM((tok_count, width), jnp.bfloat16),
            pltpu.SemaphoreType.DMA((pieces,)),
        ],
        compiler_params=pltpu.CompilerParams(vmem_limit_bytes=8 * 1024 * 1024),
    )(last, partial, w_last)
    return mixed.reshape(seq_count, tok_count, width)


def shards(tokens, norm_gain, w_in, w_out):
    peers = lax.axis_size("row") * lax.axis_size("col")
    seq_count, tok_count, _ = tokens.shape
    if seq_count == 1 and fused_fits(lax.axis_size("row"), peers, tok_count, w_in.shape[1]):
        return fused_shards(tokens, norm_gain, w_in, w_out)
    return factored_shards(tokens, norm_gain, w_in, w_out)


def solution(mesh):
    return jax.shard_map(
        shards,
        mesh=mesh,
        in_specs=(P("grp", ("row", "col"), None), P(), P(), P()),
        out_specs=P("grp", ("row", "col"), None),
        check_vma=False,
    )
```

```python
import functools
import math

import jax
import jax.numpy as jnp
import numpy as np
from jax import lax
from jax.experimental import pallas as pl
from jax.experimental.pallas import tpu as pltpu
from jax.sharding import PartitionSpec as P

GROUP_CH = 128


TWO_PI = 2.0 * math.pi
NORM_EPS = 1e-06
HIGHEST = lax.Precision.HIGHEST


def phase_tables(rows, cols, period):
    left = lax.broadcasted_iota(jnp.int32, (rows, cols), 0)
    right = lax.broadcasted_iota(jnp.int32, (rows, cols), 1)
    angles = (left * right % period).astype(jnp.float32) * (TWO_PI / period)
    return (jnp.cos(angles), jnp.sin(angles))


def rotate_by(pattern, cos_table, sin_table, real_part, imag_part):

    def apply(table, data):
        return jnp.einsum(pattern, table, data, precision=HIGHEST)

    return (
        apply(cos_table, real_part) + apply(sin_table, imag_part),
        apply(cos_table, imag_part) - apply(sin_table, real_part),
    )


def twist(real_part, imag_part, cos_table, sin_table):
    return (
        real_part * cos_table + imag_part * sin_table,
        imag_part * cos_table - real_part * sin_table,
    )


def factored_shards(tokens, norm_gain, w_in, w_out):
    seq_count, tok_count, width = tokens.shape
    feat_count = w_in.shape[1]
    row_count = lax.axis_size("row")
    col_count = lax.axis_size("col")
    block_len = tok_count * col_count
    length = block_len * row_count
    sub_feats = feat_count // row_count
    fine_count = tok_count // row_count
    item_count = seq_count * feat_count // col_count
    ortho_scale = 1.0 / math.sqrt(length * GROUP_CH)
    widened = tokens.astype(jnp.float32)
    factor = lax.rsqrt(jnp.mean(widened * widened, -1, keepdims=True) + NORM_EPS)
    normed = (widened * factor * norm_gain.astype(jnp.float32)).astype(jnp.bfloat16)
    mixin = jnp.einsum("std,df->sft", normed, w_in, preferred_element_type=jnp.float32).astype(
        jnp.bfloat16
    )
    row_cos, row_sin = phase_tables(row_count, row_count, row_count)
    chan_cos, chan_sin = phase_tables(GROUP_CH, GROUP_CH, GROUP_CH)
    stacked_shape = (seq_count, sub_feats, row_count, tok_count)
    grouped = mixin.astype(jnp.float32).reshape(
        seq_count, feat_count // GROUP_CH, GROUP_CH, tok_count
    )
    spec_real = jnp.einsum("sgqt,qm->sgmt", grouped, chan_cos, precision=HIGHEST).reshape(
        seq_count, feat_count, tok_count
    )
    spec_imag = -jnp.einsum("sgqt,qm->sgmt", grouped, chan_sin, precision=HIGHEST).reshape(
        seq_count, feat_count, tok_count
    )
    arrived = (
        lax.all_to_all(
            spec_real.astype(jnp.bfloat16), "row", split_axis=1, concat_axis=2, tiled=True
        ).astype(spec_real.dtype),
        lax.all_to_all(
            spec_imag.astype(jnp.bfloat16), "row", split_axis=1, concat_axis=2, tiled=True
        ).astype(spec_imag.dtype),
    )
    stacked_real = arrived[0].reshape(stacked_shape)
    stacked_imag = arrived[1].reshape(stacked_shape)
    real_part, imag_part = rotate_by("ka,sfat->skft", row_cos, row_sin, stacked_real, stacked_imag)
    freq_low = lax.broadcasted_iota(jnp.int32, (row_count, tok_count), 0)
    place = lax.axis_index("col") * tok_count + lax.broadcasted_iota(
        jnp.int32, (row_count, tok_count), 1
    )
    angles = (freq_low * place % length).astype(jnp.float32) * (TWO_PI / length)
    real_part, imag_part = twist(
        real_part, imag_part, jnp.cos(angles)[None, :, None, :], jnp.sin(angles)[None, :, None, :]
    )
    sending = (
        real_part.reshape(item_count, col_count, 1, tok_count),
        imag_part.reshape(item_count, col_count, 1, tok_count),
    )
    col_cos, col_sin = phase_tables(col_count, col_count, col_count)
    mid_cos, mid_sin = phase_tables(col_count, tok_count, block_len)
    tok_cos, tok_sin = phase_tables(tok_count, tok_count, tok_count)
    tok_cos = tok_cos.reshape(row_count, fine_count, tok_count)
    tok_sin = tok_sin.reshape(row_count, fine_count, tok_count)
    span_real, span_imag = rotate_by(
        "uc,qct->qut",
        col_cos,
        col_sin,
        lax.all_to_all(
            sending[0].astype(jnp.bfloat16), "col", split_axis=1, concat_axis=2, tiled=True
        ).astype(jnp.float32)[:, 0],
        lax.all_to_all(
            sending[1].astype(jnp.bfloat16), "col", split_axis=1, concat_axis=2, tiled=True
        ).astype(jnp.float32)[:, 0],
    )
    span_real, span_imag = twist(span_real, span_imag, mid_cos, mid_sin)
    span_real, span_imag = rotate_by("rjt,qut->rjuq", tok_cos, tok_sin, span_real, span_imag)
    owner_shape = (row_count, col_count, fine_count, span_real.shape[-1], 1)
    span_real, span_imag = (span_real.reshape(owner_shape), span_imag.reshape(owner_shape))
    rounded = (span_real * ortho_scale).astype(jnp.bfloat16)
    returned = lax.all_to_all(rounded, "col", split_axis=1, concat_axis=4, tiled=True)
    layout = (row_count, fine_count, seq_count, row_count, sub_feats)
    spectrum = lax.all_to_all(
        returned.reshape(layout), "row", split_axis=0, concat_axis=4, tiled=True
    )
    spectrum = spectrum.reshape(fine_count, seq_count, row_count, feat_count)
    mixed = jnp.einsum("jskf,fd->sjkd", spectrum, w_out, preferred_element_type=jnp.float32).astype(
        jnp.bfloat16
    )
    return mixed.reshape(seq_count, fine_count * row_count, width)


CHUNKS = 4
LANES = 128
MESH = pl.DeviceIdType.MESH


def host_spots(row_count, col_count):
    rows = (row_count // 2 - 1, row_count // 2)
    return [(row, col) for row in rows for col in range(1, col_count, 2)]


def fused_fits(row_count, col_count, tok_count, feat_count):
    peers = row_count * col_count
    return (
        row_count >= 4
        and peers == 16
        and tok_count == LANES
        and GROUP_CH == LANES
        and feat_count == GROUP_CH * len(host_spots(row_count, col_count))
        and feat_count > GROUP_CH
    )


def row_slots(peers):
    slots = [0, peers // 2]
    for a in range(1, peers // 2):
        slots += [a, peers - a]
    return slots


def host_tables(peers, tok_count):
    length = peers * tok_count
    half = GROUP_CH // 2
    q = np.arange(GROUP_CH)[:, None]
    m = np.arange(half)[None, :]
    chan = np.zeros((GROUP_CH, GROUP_CH))
    chan[:, :half] = np.cos(2 * np.pi * (q * m % GROUP_CH) / GROUP_CH)
    chan[:, half:] = -np.sin(2 * np.pi * (q * m % GROUP_CH) / GROUP_CH)
    chan[:, half] = np.cos(np.pi * q[:, 0])
    t = np.arange(tok_count)[None, :]
    b = np.arange(tok_count)[:, None]
    scale = 1.0 / math.sqrt(length * GROUP_CH)
    mid = np.zeros((peers, tok_count, 2, tok_count))
    for a in range(peers):
        angle = 2 * np.pi * (t * (peers * b + a) % length) / length
        mid[a, :, 0] = np.cos(angle) * scale
        mid[a, :, 1] = -np.sin(angle) * scale * (1 if a <= peers // 2 else -1)
    mid = mid.reshape(peers, tok_count, 2 * tok_count)
    fold = np.zeros((GROUP_CH, GROUP_CH))
    fold[0, 0] = 1
    fold[half, half] = 1
    for a in range(1, half):
        fold[a, a] = 1
        fold[a, GROUP_CH - a] = 1
        fold[half + a, a] = 1
        fold[half + a, GROUP_CH - a] = -1
    return [jnp.asarray(x, jnp.bfloat16) for x in (chan, mid, fold)]


def short_transform(x):
    r = math.sqrt(0.5)
    c1, s1 = math.cos(math.pi / 8), math.sin(math.pi / 8)
    e = [x[s] + x[s + 8] for s in range(8)]
    o = [x[s] - x[s + 8] for s in range(8)]
    p04, n04 = e[0] + e[4], e[0] - e[4]
    p26, n26 = e[2] + e[6], e[2] - e[6]
    p15, n15 = e[1] + e[5], e[1] - e[5]
    p37, n37 = e[3] + e[7], e[3] - e[7]
    low, high = p04 + p26, p15 + p37
    even_cos = (n15 - n37) * r
    even_sin = (n15 + n37) * r
    found = {
        0: (low + high, None),
        8: (low - high, None),
        4: (p04 - p26, p15 - p37),
        2: (n04 + even_cos, even_sin + n26),
        6: (n04 - even_cos, even_sin - n26),
    }
    f1, f2, f3 = o[1] - o[7], (o[2] - o[6]) * r, o[3] - o[5]
    g1, g2, g3 = o[1] + o[7], (o[2] + o[6]) * r, o[3] + o[5]
    up, down = o[0] + f2, o[0] - f2
    one, two = f1 * c1 + f3 * s1, f1 * s1 - f3 * c1
    cosines = {1: up + one, 7: up - one, 3: down + two, 5: down - two}
    plus, minus = g2 + o[4], g2 - o[4]
    three, four = g1 * s1 + g3 * c1, g1 * c1 - g3 * s1
    sines = {1: three + plus, 7: three - plus, 3: four + minus, 5: four - minus}
    for a in (1, 3, 5, 7):
        found[a] = (cosines[a], sines[a])
    return found


def fused_kernel(
    shape,
    tokens_hbm,
    gain_hbm,
    w_in_hbm,
    chan_hbm,
    mid_hbm,
    fold_hbm,
    w_out_hbm,
    last_ref,
    partial_ref,
    w_last,
    tokens,
    gain,
    w_in,
    chan,
    mid,
    fold,
    w_out,
    w_first,
    natural,
    first_out,
    first_in,
    blocks,
    second_out,
    second_in,
    load_sem,
    send_sem,
    recv_a,
    recv_b,
):
    row_count, col_count = shape
    peers = row_count * col_count
    tok_count, width = tokens.shape
    feat_count = w_in.shape[1]
    fine = tok_count // peers
    groups = feat_count // GROUP_CH
    half = GROUP_CH // 2
    spots = host_spots(row_count, col_count)
    hosts = [r * col_count + c for r, c in spots]
    row, col = lax.axis_index("row"), lax.axis_index("col")
    me = row * col_count + col
    is_host = me == hosts[0]
    group = jnp.int32(0)
    for g in range(1, groups):
        is_host = is_host | (me == hosts[g])
        group = group + jnp.where(me == hosts[g], g, 0)

    def device(index):
        return {"row": index // col_count, "col": index % col_count}

    load_tokens = pltpu.make_async_copy(tokens_hbm, tokens, load_sem.at[0])
    load_gain = pltpu.make_async_copy(gain_hbm, gain, load_sem.at[1])
    load_chan = pltpu.make_async_copy(chan_hbm, chan, load_sem.at[2])
    load_mid = pltpu.make_async_copy(mid_hbm, mid, load_sem.at[3])
    load_fold = pltpu.make_async_copy(fold_hbm, fold, load_sem.at[4])
    load_out = pltpu.make_async_copy(w_out_hbm, w_out, load_sem.at[5])
    size = feat_count // CHUNKS
    load_w = []
    for c in range(CHUNKS):
        at = (slice(None), pl.ds(c * size, size))
        load_w.append(pltpu.make_async_copy(w_in_hbm.at[at], w_in.at[at], load_sem.at[6 + c]))
    load_tokens.start()
    load_gain.start()
    load_w[0].start()
    load_chan.start()
    for load in load_w[1:]:
        load.start()

    barrier = pltpu.get_barrier_semaphore()

    @pl.when(is_host)
    def _():
        for step in range(1, peers):
            target = lax.rem(me + step, peers)
            pl.semaphore_signal(
                barrier,
                inc=1,
                device_id={"row": target // col_count, "col": lax.rem(target, col_count)},
                device_id_type=MESH,
            )

    load_tokens.wait()
    load_gain.wait()
    scaled = tokens[...] * gain[...].reshape(1, width)
    widened = tokens[...].astype(jnp.float32)
    factor = lax.rsqrt(jnp.mean(widened * widened, -1, keepdims=True) + NORM_EPS)
    for c in range(CHUNKS):
        load_w[c].wait()
        if c == CHUNKS - 1:
            load_fold.start()

            @pl.when(is_host)
            def _():
                load_mid.start()

            load_out.start()
        mixin = jnp.dot(
            scaled, w_in[:, c * size : (c + 1) * size], preferred_element_type=jnp.float32
        )
        mixin = (mixin * factor).astype(jnp.bfloat16)
        if c == 0:
            load_chan.wait()
        for i in range(size // GROUP_CH):
            g = c * (size // GROUP_CH) + i
            first_out[g] = jnp.dot(
                mixin[:, i * GROUP_CH : (i + 1) * GROUP_CH],
                chan[...],
                preferred_element_type=jnp.float32,
            ).astype(jnp.bfloat16)
            if g == 0:

                @pl.when(is_host)
                def _():
                    pl.semaphore_wait(barrier, groups - 1)

                @pl.when(jnp.logical_not(is_host))
                def _():
                    pl.semaphore_wait(barrier, groups)

            @pl.when(me != hosts[g])
            def _():
                pltpu.make_async_remote_copy(
                    src_ref=first_out.at[g],
                    dst_ref=first_in.at[me],
                    send_sem=send_sem.at[0],
                    recv_sem=recv_a.at[0],
                    device_id=device(hosts[g]),
                    device_id_type=MESH,
                ).start()

            @pl.when(me == hosts[g])
            def _():
                first_in[me] = first_out[g]

    load_fold.wait()
    load_out.wait()
    for g in range(groups):
        span = slice(g * GROUP_CH, (g + 1) * GROUP_CH)
        folded = jnp.dot(fold[...], w_out[span, :], preferred_element_type=jnp.float32)
        if g < groups - 1:
            w_first[span, :] = folded.astype(jnp.bfloat16)
        else:
            w_last[...] = folded.astype(jnp.bfloat16)

    slots = row_slots(peers)

    @pl.when(is_host)
    def _():
        load_mid.wait()
        rest = first_in.at[pl.ds(0, peers - 1)]
        pltpu.make_async_copy(rest, rest, recv_a.at[0]).wait()
        step = 16
        cosine_lane = lax.broadcasted_iota(jnp.int32, (step, LANES), 1) <= half
        for top in range(0, tok_count, step):
            arrived = [first_in[s, top : top + step].astype(jnp.float32) for s in range(peers)]
            for a, (cosine, sine) in short_transform(arrived).items():
                if sine is None:
                    upper = jnp.where(cosine_lane, cosine, 0.0)
                    lower = jnp.where(cosine_lane, 0.0, -cosine)
                else:
                    upper = jnp.where(cosine_lane, cosine, sine)
                    lower = jnp.where(cosine_lane, sine, -cosine)
                blocks[a, top : top + step] = upper.astype(jnp.bfloat16)
                blocks[a, tok_count + top : tok_count + top + step] = lower.astype(jnp.bfloat16)
        for i in range(0, peers, 2):
            pair = [
                jnp.dot(
                    mid[a], blocks[min(a, peers - a)], preferred_element_type=jnp.float32
                ).reshape(peers, fine, LANES)
                for a in slots[i : i + 2]
            ]
            second_out[:, i * fine : (i + 2) * fine, :] = jnp.concatenate(pair, axis=1).astype(
                jnp.bfloat16
            )

        def send(target):
            pltpu.make_async_remote_copy(
                src_ref=second_out.at[target],
                dst_ref=second_in.at[group],
                send_sem=send_sem.at[1],
                recv_sem=recv_b.at[group],
                device_id={"row": target // col_count, "col": lax.rem(target, col_count)},
                device_id_type=MESH,
            ).start()

        low = spots[0][0]
        for i in range(low):
            for edge in (i, row_count - 1 - i):
                for c in range(col_count):
                    send(edge * col_count + c)
        other = low * 2 + 1 - row
        for c in range(col_count):
            send(other * col_count + c)
        for shift in range(1, col_count):
            send(row * col_count + lax.rem(col + shift, col_count))
        second_in[group] = second_out[me]

    @pl.when(is_host)
    def _():
        sent = first_out.at[pl.ds(0, groups - 1)]
        pltpu.make_async_copy(sent, sent, send_sem.at[0]).wait()

    @pl.when(jnp.logical_not(is_host))
    def _():
        pltpu.make_async_copy(first_out, first_out, send_sem.at[0]).wait()

    flipped = jnp.where(lax.broadcasted_iota(jnp.int32, (fine, LANES), 1) > half, -1.0, 1.0)

    def collect(g):
        @pl.when(me != hosts[g])
        def _():
            pltpu.make_async_copy(second_in.at[g], second_in.at[g], recv_b.at[g]).wait()

        for i, a in enumerate(slots):
            part = second_in[g, i * fine : (i + 1) * fine].astype(jnp.float32)
            if a > peers // 2:
                part = part * flipped
            natural[g, pl.ds(a, fine, stride=peers), :] = part
        return natural[g].astype(jnp.bfloat16)

    def project(g, value):
        return jnp.dot(
            value,
            w_first[g * GROUP_CH : (g + 1) * GROUP_CH, :],
            preferred_element_type=jnp.float32,
        )

    for g in range(groups - 1):
        term = project(g, collect(g))
        if g == 0:
            partial_ref[...] = term
        else:
            partial_ref[...] += term

    @pl.when(is_host)
    def _():
        sent = second_out.at[pl.ds(0, peers - 1)]
        pltpu.make_async_copy(sent, sent, send_sem.at[1]).wait()

    last_ref[...] = collect(groups - 1)


def project_kernel(chunks, last, partial, w_last, out_hbm, staged, sem):
    size = w_last.shape[1] // chunks
    for i in range(chunks):
        lanes = slice(i * size, (i + 1) * size)
        staged[:, lanes] = (
            partial[:, lanes]
            + jnp.dot(last[...], w_last[:, lanes], preferred_element_type=jnp.float32)
        ).astype(staged.dtype)
        span = pl.ds(i * size, size)
        pltpu.make_async_copy(staged.at[:, span], out_hbm.at[:, span], sem).start()
    pltpu.make_async_copy(staged, out_hbm, sem).wait()


def fused_shards(tokens, norm_gain, w_in, w_out):
    seq_count, tok_count, width = tokens.shape
    feat_count = w_in.shape[1]
    shape = (lax.axis_size("row"), lax.axis_size("col"))
    peers = shape[0] * shape[1]
    groups = feat_count // GROUP_CH
    tables = host_tables(peers, tok_count)
    operands = [tokens.reshape(tok_count, width), norm_gain, w_in, *tables, w_out]
    held = [pltpu.VMEM(x.shape, x.dtype) for x in operands]
    last, partial, w_last = pl.pallas_call(
        functools.partial(fused_kernel, shape),
        out_shape=(
            pltpu.VMEM((tok_count, GROUP_CH), jnp.bfloat16),
            pltpu.VMEM((tok_count, width), jnp.float32),
            pltpu.VMEM((GROUP_CH, width), jnp.bfloat16),
        ),
        in_specs=[pl.BlockSpec(memory_space=pltpu.HBM)] * len(operands),
        out_specs=(pl.BlockSpec(memory_space=pltpu.VMEM),) * 3,
        scratch_shapes=held
        + [
            pltpu.VMEM((feat_count - GROUP_CH, width), jnp.bfloat16),
            pltpu.VMEM((groups, tok_count, GROUP_CH), jnp.float32),
            pltpu.VMEM((groups, tok_count, GROUP_CH), jnp.bfloat16),
            pltpu.VMEM((peers, tok_count, GROUP_CH), jnp.bfloat16),
            pltpu.VMEM((peers // 2 + 1, 2 * tok_count, GROUP_CH), jnp.bfloat16),
            pltpu.VMEM((peers, tok_count, GROUP_CH), jnp.bfloat16),
            pltpu.VMEM((groups, tok_count, GROUP_CH), jnp.bfloat16),
            pltpu.SemaphoreType.DMA((6 + CHUNKS,)),
            pltpu.SemaphoreType.DMA((2,)),
            pltpu.SemaphoreType.DMA((1,)),
            pltpu.SemaphoreType.DMA((groups,)),
        ],
        compiler_params=pltpu.CompilerParams(
            collective_id=0, has_side_effects=True, vmem_limit_bytes=62_000_000
        ),
    )(*operands)
    pieces = max(1, width // 512)
    mixed = pl.pallas_call(
        functools.partial(project_kernel, pieces),
        out_shape=jax.ShapeDtypeStruct((tok_count, width), jnp.bfloat16),
        in_specs=[pl.BlockSpec(memory_space=pltpu.VMEM)] * 3,
        out_specs=pl.BlockSpec(memory_space=pltpu.HBM),
        scratch_shapes=[pltpu.VMEM((tok_count, width), jnp.bfloat16), pltpu.SemaphoreType.DMA],
        compiler_params=pltpu.CompilerParams(vmem_limit_bytes=8 * 1024 * 1024),
    )(last, partial, w_last)
    return mixed.reshape(seq_count, tok_count, width)


def shards(tokens, norm_gain, w_in, w_out):
    seq_count, tok_count, _ = tokens.shape
    shape = (lax.axis_size("row"), lax.axis_size("col"))
    if seq_count == 1 and fused_fits(*shape, tok_count, w_in.shape[1]):
        return fused_shards(tokens, norm_gain, w_in, w_out)
    return factored_shards(tokens, norm_gain, w_in, w_out)


def solution(mesh):
    return jax.shard_map(
        shards,
        mesh=mesh,
        in_specs=(P("grp", ("row", "col"), None), P(), P(), P()),
        out_specs=P("grp", ("row", "col"), None),
        check_vma=False,
    )
```

```python
import functools
import math

import jax
import jax.numpy as jnp
import numpy as np
from jax import lax
from jax.experimental import pallas as pl
from jax.experimental.pallas import tpu as pltpu
from jax.sharding import PartitionSpec as P

GROUP_CH = 128


TWO_PI = 2.0 * math.pi
NORM_EPS = 1e-06
HIGHEST = lax.Precision.HIGHEST


def phase_tables(rows, cols, period):
    left = lax.broadcasted_iota(jnp.int32, (rows, cols), 0)
    right = lax.broadcasted_iota(jnp.int32, (rows, cols), 1)
    angles = (left * right % period).astype(jnp.float32) * (TWO_PI / period)
    return (jnp.cos(angles), jnp.sin(angles))


def rotate_by(pattern, cos_table, sin_table, real_part, imag_part):

    def apply(table, data):
        return jnp.einsum(pattern, table, data, precision=HIGHEST)

    return (
        apply(cos_table, real_part) + apply(sin_table, imag_part),
        apply(cos_table, imag_part) - apply(sin_table, real_part),
    )


def twist(real_part, imag_part, cos_table, sin_table):
    return (
        real_part * cos_table + imag_part * sin_table,
        imag_part * cos_table - real_part * sin_table,
    )


def factored_shards(tokens, norm_gain, w_in, w_out):
    seq_count, tok_count, width = tokens.shape
    feat_count = w_in.shape[1]
    row_count = lax.axis_size("row")
    col_count = lax.axis_size("col")
    block_len = tok_count * col_count
    length = block_len * row_count
    sub_feats = feat_count // row_count
    fine_count = tok_count // row_count
    item_count = seq_count * feat_count // col_count
    ortho_scale = 1.0 / math.sqrt(length * GROUP_CH)
    widened = tokens.astype(jnp.float32)
    factor = lax.rsqrt(jnp.mean(widened * widened, -1, keepdims=True) + NORM_EPS)
    normed = (widened * factor * norm_gain.astype(jnp.float32)).astype(jnp.bfloat16)
    mixin = jnp.einsum("std,df->sft", normed, w_in, preferred_element_type=jnp.float32).astype(
        jnp.bfloat16
    )
    row_cos, row_sin = phase_tables(row_count, row_count, row_count)
    chan_cos, chan_sin = phase_tables(GROUP_CH, GROUP_CH, GROUP_CH)
    stacked_shape = (seq_count, sub_feats, row_count, tok_count)
    grouped = mixin.astype(jnp.float32).reshape(
        seq_count, feat_count // GROUP_CH, GROUP_CH, tok_count
    )
    spec_real = jnp.einsum("sgqt,qm->sgmt", grouped, chan_cos, precision=HIGHEST).reshape(
        seq_count, feat_count, tok_count
    )
    spec_imag = -jnp.einsum("sgqt,qm->sgmt", grouped, chan_sin, precision=HIGHEST).reshape(
        seq_count, feat_count, tok_count
    )
    arrived = (
        lax.all_to_all(
            spec_real.astype(jnp.bfloat16), "row", split_axis=1, concat_axis=2, tiled=True
        ).astype(spec_real.dtype),
        lax.all_to_all(
            spec_imag.astype(jnp.bfloat16), "row", split_axis=1, concat_axis=2, tiled=True
        ).astype(spec_imag.dtype),
    )
    stacked_real = arrived[0].reshape(stacked_shape)
    stacked_imag = arrived[1].reshape(stacked_shape)
    real_part, imag_part = rotate_by("ka,sfat->skft", row_cos, row_sin, stacked_real, stacked_imag)
    freq_low = lax.broadcasted_iota(jnp.int32, (row_count, tok_count), 0)
    place = lax.axis_index("col") * tok_count + lax.broadcasted_iota(
        jnp.int32, (row_count, tok_count), 1
    )
    angles = (freq_low * place % length).astype(jnp.float32) * (TWO_PI / length)
    real_part, imag_part = twist(
        real_part, imag_part, jnp.cos(angles)[None, :, None, :], jnp.sin(angles)[None, :, None, :]
    )
    sending = (
        real_part.reshape(item_count, col_count, 1, tok_count),
        imag_part.reshape(item_count, col_count, 1, tok_count),
    )
    col_cos, col_sin = phase_tables(col_count, col_count, col_count)
    mid_cos, mid_sin = phase_tables(col_count, tok_count, block_len)
    tok_cos, tok_sin = phase_tables(tok_count, tok_count, tok_count)
    tok_cos = tok_cos.reshape(row_count, fine_count, tok_count)
    tok_sin = tok_sin.reshape(row_count, fine_count, tok_count)
    span_real, span_imag = rotate_by(
        "uc,qct->qut",
        col_cos,
        col_sin,
        lax.all_to_all(
            sending[0].astype(jnp.bfloat16), "col", split_axis=1, concat_axis=2, tiled=True
        ).astype(jnp.float32)[:, 0],
        lax.all_to_all(
            sending[1].astype(jnp.bfloat16), "col", split_axis=1, concat_axis=2, tiled=True
        ).astype(jnp.float32)[:, 0],
    )
    span_real, span_imag = twist(span_real, span_imag, mid_cos, mid_sin)
    span_real, span_imag = rotate_by("rjt,qut->rjuq", tok_cos, tok_sin, span_real, span_imag)
    owner_shape = (row_count, col_count, fine_count, span_real.shape[-1], 1)
    span_real, span_imag = (span_real.reshape(owner_shape), span_imag.reshape(owner_shape))
    rounded = (span_real * ortho_scale).astype(jnp.bfloat16)
    returned = lax.all_to_all(rounded, "col", split_axis=1, concat_axis=4, tiled=True)
    layout = (row_count, fine_count, seq_count, row_count, sub_feats)
    spectrum = lax.all_to_all(
        returned.reshape(layout), "row", split_axis=0, concat_axis=4, tiled=True
    )
    spectrum = spectrum.reshape(fine_count, seq_count, row_count, feat_count)
    mixed = jnp.einsum("jskf,fd->sjkd", spectrum, w_out, preferred_element_type=jnp.float32).astype(
        jnp.bfloat16
    )
    return mixed.reshape(seq_count, fine_count * row_count, width)


CHUNKS = 4
LATE = 2
LANES = 128
MESH = pl.DeviceIdType.MESH


def host_spots(row_count):
    low, high = row_count // 2 - 1, row_count // 2
    return [(low, 1), (low, 3), (high, 3), (high, 1)]


def fused_fits(row_count, col_count, tok_count, feat_count):
    return (
        row_count == 4
        and col_count == 4
        and tok_count == LANES
        and GROUP_CH == LANES
        and feat_count == GROUP_CH * 4
    )


def row_slots(peers):
    pairs = [(0, peers // 2)] + [(a, peers - a) for a in range(1, peers // 2)]
    return [a for parity in (0, 1) for pair in pairs if pair[0] % 2 == parity for a in pair]


def host_tables(peers, tok_count):
    length = peers * tok_count
    half = GROUP_CH // 2
    q = np.arange(GROUP_CH)[:, None]
    m = np.arange(half)[None, :]
    chan = np.zeros((GROUP_CH, GROUP_CH))
    chan[:, :half] = np.cos(2 * np.pi * (q * m % GROUP_CH) / GROUP_CH)
    chan[:, half:] = -np.sin(2 * np.pi * (q * m % GROUP_CH) / GROUP_CH)
    chan[:, half] = np.cos(np.pi * q[:, 0])
    t = np.arange(tok_count)[None, :]
    b = np.arange(tok_count)[:, None]
    scale = 1.0 / math.sqrt(length * GROUP_CH)
    mid = np.zeros((peers, tok_count, 2, tok_count))
    for a in range(peers):
        angle = 2 * np.pi * (t * (peers * b + a) % length) / length
        mid[a, :, 0] = np.cos(angle) * scale
        mid[a, :, 1] = -np.sin(angle) * scale * (1 if a <= peers // 2 else -1)
    mid = mid.reshape(peers, tok_count, 2 * tok_count)[row_slots(peers)]
    fold = np.zeros((GROUP_CH, GROUP_CH))
    fold[0, 0] = 1
    fold[half, half] = 1
    for a in range(1, half):
        fold[a, a] = 1
        fold[a, GROUP_CH - a] = 1
        fold[half + a, a] = 1
        fold[half + a, GROUP_CH - a] = -1
    return [jnp.asarray(x, jnp.bfloat16) for x in (np.stack([chan, fold]), mid)]


def even_transform(x):
    r = math.sqrt(0.5)
    e = [(x[s] + x[s + 8]).astype(jnp.float32) for s in range(8)]
    p04, n04 = e[0] + e[4], e[0] - e[4]
    p26, n26 = e[2] + e[6], e[2] - e[6]
    p15, n15 = e[1] + e[5], e[1] - e[5]
    p37, n37 = e[3] + e[7], e[3] - e[7]
    low, high = p04 + p26, p15 + p37
    even_cos = (n15 - n37) * r
    even_sin = (n15 + n37) * r
    return {
        0: (low + high, None),
        8: (low - high, None),
        4: (p04 - p26, p15 - p37),
        2: (n04 + even_cos, even_sin + n26),
        6: (n04 - even_cos, even_sin - n26),
    }


def odd_transform(x):
    r = math.sqrt(0.5)
    c1, s1 = math.cos(math.pi / 8), math.sin(math.pi / 8)
    o = [(x[s] - x[s + 8]).astype(jnp.float32) for s in range(8)]
    f1, f2, f3 = o[1] - o[7], (o[2] - o[6]) * r, o[3] - o[5]
    g1, g2, g3 = o[1] + o[7], (o[2] + o[6]) * r, o[3] + o[5]
    up, down = o[0] + f2, o[0] - f2
    one, two = f1 * c1 + f3 * s1, f1 * s1 - f3 * c1
    plus, minus = g2 + o[4], g2 - o[4]
    three, four = g1 * s1 + g3 * c1, g1 * c1 - g3 * s1
    return {
        1: (up + one, three + plus),
        7: (up - one, three - plus),
        3: (down + two, four + minus),
        5: (down - two, four - minus),
    }


def fused_kernel(
    shape,
    tokens_hbm,
    gain_hbm,
    w_in_hbm,
    small_hbm,
    mid_hbm,
    w_out_hbm,
    last_ref,
    partial_ref,
    w_last,
    tokens,
    gain,
    w_in,
    small,
    mid,
    w_out,
    w_first,
    natural,
    first_out,
    first_in,
    blocks,
    second_out,
    second_in,
    load_sem,
    send_sem,
    recv_a,
    recv_b,
):
    row_count, col_count = shape
    peers = row_count * col_count
    tok_count, width = tokens.shape
    feat_count = w_in.shape[1]
    fine = tok_count // peers
    groups = feat_count // GROUP_CH
    half = GROUP_CH // 2
    hosts = [r * col_count + c for r, c in host_spots(row_count)]
    row, col = lax.axis_index("row"), lax.axis_index("col")
    me = row * col_count + col
    is_host = me == hosts[0]
    for spot in hosts[1:]:
        is_host = is_host | (me == spot)

    def device(index):
        return {"row": index // col_count, "col": index % col_count}

    load_tokens = pltpu.make_async_copy(tokens_hbm, tokens, load_sem.at[0])
    load_gain = pltpu.make_async_copy(gain_hbm, gain, load_sem.at[1])
    load_small = pltpu.make_async_copy(small_hbm, small, load_sem.at[2])
    load_mid = pltpu.make_async_copy(mid_hbm, mid, load_sem.at[3])
    load_out = pltpu.make_async_copy(w_out_hbm, w_out, load_sem.at[4])
    size = feat_count // CHUNKS
    load_w = []
    for c in range(CHUNKS):
        at = (slice(None), pl.ds(c * size, size))
        load_w.append(pltpu.make_async_copy(w_in_hbm.at[at], w_in.at[at], load_sem.at[5 + c]))
    load_tokens.start()
    load_gain.start()
    load_w[0].start()
    load_small.start()
    for load in load_w[1:]:
        load.start()

    barrier = pltpu.get_barrier_semaphore()

    @pl.when(is_host)
    def _():
        for step in range(1, peers):
            target = lax.rem(me + step, peers)
            pl.semaphore_signal(
                barrier,
                inc=1,
                device_id={"row": target // col_count, "col": lax.rem(target, col_count)},
                device_id_type=MESH,
            )

    load_tokens.wait()
    load_gain.wait()
    scaled = tokens[...] * gain[...].reshape(1, width)
    widened = tokens[...].astype(jnp.float32)
    factor = lax.rsqrt(jnp.mean(widened * widened, -1, keepdims=True) + NORM_EPS)
    for c in range(CHUNKS):
        load_w[c].wait()
        if c == CHUNKS - 1:

            @pl.when(is_host)
            def _():
                load_mid.start()

            load_out.start()
        mixin = jnp.dot(
            scaled, w_in[:, c * size : (c + 1) * size], preferred_element_type=jnp.float32
        )
        mixin = (mixin * factor).astype(jnp.bfloat16)
        if c == 0:
            load_small.wait()
        for i in range(size // GROUP_CH):
            g = c * (size // GROUP_CH) + i
            first_out[g] = jnp.dot(
                mixin[:, i * GROUP_CH : (i + 1) * GROUP_CH],
                small[0],
                preferred_element_type=jnp.float32,
            ).astype(jnp.bfloat16)
            if g == 0:

                @pl.when(is_host)
                def _():
                    pl.semaphore_wait(barrier, groups - 1)

                @pl.when(jnp.logical_not(is_host))
                def _():
                    pl.semaphore_wait(barrier, groups)

            spot = hosts[g]

            @pl.when(me != spot)
            def _():
                pltpu.make_async_remote_copy(
                    src_ref=first_out.at[g],
                    dst_ref=first_in.at[me],
                    send_sem=send_sem.at[0],
                    recv_sem=recv_a.at[0],
                    device_id=device(spot),
                    device_id_type=MESH,
                ).start()

            @pl.when(me == spot)
            def _():
                first_in[me] = first_out[g]

    load_out.wait()
    for g in range(groups):
        span = slice(g * GROUP_CH, (g + 1) * GROUP_CH)
        folded = jnp.dot(small[1], w_out[span, :], preferred_element_type=jnp.float32)
        if g < groups - LATE:
            w_first[span, :] = folded.astype(jnp.bfloat16)
        else:
            at = (g - groups + LATE) * GROUP_CH
            w_last[at : at + GROUP_CH, :] = folded.astype(jnp.bfloat16)

    slots = row_slots(peers)

    @pl.when(is_host)
    def _():
        load_mid.wait()
        rest = first_in.at[pl.ds(0, peers - 1)]
        pltpu.make_async_copy(rest, rest, recv_a.at[0]).wait()
        step = 16
        cosine_lane = lax.broadcasted_iota(jnp.int16, (step, LANES), 1) <= half
        zero = jnp.zeros((step, LANES), jnp.bfloat16)
        for parity, transform in enumerate((even_transform, odd_transform)):
            for top in range(0, tok_count, step):
                arrived = [first_in[s, top : top + step] for s in range(peers)]
                for a, (cosine, sine) in transform(arrived).items():
                    cosine = cosine.astype(jnp.bfloat16)
                    sine = zero if sine is None else sine.astype(jnp.bfloat16)
                    blocks[a, top : top + step] = jnp.where(cosine_lane, cosine, sine)
                    blocks[a, tok_count + top : tok_count + top + step] = jnp.where(
                        cosine_lane, sine, -cosine
                    )
            for i in range(parity * peers // 2, (parity + 1) * peers // 2, 2):
                pair = [
                    jnp.dot(
                        mid[i + n], blocks[min(a, peers - a)], preferred_element_type=jnp.float32
                    ).reshape(peers, fine, LANES)
                    for n, a in enumerate(slots[i : i + 2])
                ]
                second_out[:, i * fine : (i + 2) * fine, :] = jnp.concatenate(pair, axis=1).astype(
                    jnp.bfloat16
                )

    served = [0, row_count - 1, *range(1, row_count - 1)]
    served = [r * col_count + c for r in served for c in range(col_count)]
    for g, spot in enumerate(hosts):

        @pl.when(me == spot)
        def _():
            for target in served:
                if target != spot:
                    pltpu.make_async_remote_copy(
                        src_ref=second_out.at[target],
                        dst_ref=second_in.at[g],
                        send_sem=send_sem.at[1],
                        recv_sem=recv_b.at[g // LATE],
                        device_id=device(target),
                        device_id_type=MESH,
                    ).start()
            second_in[g] = second_out[spot]

    @pl.when(is_host)
    def _():
        sent = first_out.at[pl.ds(0, groups - 1)]
        pltpu.make_async_copy(sent, sent, send_sem.at[0]).wait()

    @pl.when(jnp.logical_not(is_host))
    def _():
        pltpu.make_async_copy(first_out, first_out, send_sem.at[0]).wait()

    flipped = jnp.where(lax.broadcasted_iota(jnp.int32, (fine, LANES), 1) > half, -1.0, 1.0)

    def arrive(pair):
        own = (me == hosts[pair * LATE]) | (me == hosts[pair * LATE + 1])

        @pl.when(own)
        def _():
            one = second_in.at[pair * LATE]
            pltpu.make_async_copy(one, one, recv_b.at[pair]).wait()

        @pl.when(jnp.logical_not(own))
        def _():
            both = second_in.at[pl.ds(pair * LATE, LATE)]
            pltpu.make_async_copy(both, both, recv_b.at[pair]).wait()

    def collect(g):
        for i, a in enumerate(slots):
            part = second_in[g, i * fine : (i + 1) * fine].astype(jnp.float32)
            if a > peers // 2:
                part = part * flipped
            natural[g, pl.ds(a, fine, stride=peers), :] = part
        return natural[g].astype(jnp.bfloat16)

    arrive(0)
    early = [collect(g) for g in range(LATE)]
    partial_ref[...] = jnp.dot(
        jnp.concatenate(early, axis=1), w_first[...], preferred_element_type=jnp.float32
    )
    arrive(1)
    for g in range(LATE):
        last_ref[:, g * GROUP_CH : (g + 1) * GROUP_CH] = collect(LATE + g)

    @pl.when(is_host)
    def _():
        sent = second_out.at[pl.ds(0, peers - 1)]
        pltpu.make_async_copy(sent, sent, send_sem.at[1]).wait()


def project_kernel(chunks, last, partial, w_last, out_hbm, staged, sem):
    size = w_last.shape[1] // chunks
    for i in range(chunks):
        lanes = slice(i * size, (i + 1) * size)
        staged[:, lanes] = (
            partial[:, lanes]
            + jnp.dot(last[...], w_last[:, lanes], preferred_element_type=jnp.float32)
        ).astype(staged.dtype)
        span = pl.ds(i * size, size)
        pltpu.make_async_copy(staged.at[:, span], out_hbm.at[:, span], sem).start()
    pltpu.make_async_copy(staged, out_hbm, sem).wait()


def fused_shards(tokens, norm_gain, w_in, w_out):
    seq_count, tok_count, width = tokens.shape
    feat_count = w_in.shape[1]
    shape = (lax.axis_size("row"), lax.axis_size("col"))
    peers = shape[0] * shape[1]
    groups = feat_count // GROUP_CH
    tables = host_tables(peers, tok_count)
    operands = [tokens.reshape(tok_count, width), norm_gain, w_in, *tables, w_out]
    held = [pltpu.VMEM(x.shape, x.dtype) for x in operands]
    last, partial, w_last = pl.pallas_call(
        functools.partial(fused_kernel, shape),
        out_shape=(
            pltpu.VMEM((tok_count, LATE * GROUP_CH), jnp.bfloat16),
            pltpu.VMEM((tok_count, width), jnp.float32),
            pltpu.VMEM((LATE * GROUP_CH, width), jnp.bfloat16),
        ),
        in_specs=[pl.BlockSpec(memory_space=pltpu.HBM)] * len(operands),
        out_specs=(pl.BlockSpec(memory_space=pltpu.VMEM),) * 3,
        scratch_shapes=held
        + [
            pltpu.VMEM((feat_count - LATE * GROUP_CH, width), jnp.bfloat16),
            pltpu.VMEM((groups, tok_count, GROUP_CH), jnp.float32),
            pltpu.VMEM((groups, tok_count, GROUP_CH), jnp.bfloat16),
            pltpu.VMEM((peers, tok_count, GROUP_CH), jnp.bfloat16),
            pltpu.VMEM((peers // 2 + 1, 2 * tok_count, GROUP_CH), jnp.bfloat16),
            pltpu.VMEM((peers, tok_count, GROUP_CH), jnp.bfloat16),
            pltpu.VMEM((groups, tok_count, GROUP_CH), jnp.bfloat16),
            pltpu.SemaphoreType.DMA((5 + CHUNKS,)),
            pltpu.SemaphoreType.DMA((2,)),
            pltpu.SemaphoreType.DMA((1,)),
            pltpu.SemaphoreType.DMA((groups // LATE,)),
        ],
        compiler_params=pltpu.CompilerParams(
            collective_id=0, has_side_effects=True, vmem_limit_bytes=62_000_000
        ),
    )(*operands)
    pieces = max(1, width // 512)
    mixed = pl.pallas_call(
        functools.partial(project_kernel, pieces),
        out_shape=jax.ShapeDtypeStruct((tok_count, width), jnp.bfloat16),
        in_specs=[pl.BlockSpec(memory_space=pltpu.VMEM)] * 3,
        out_specs=pl.BlockSpec(memory_space=pltpu.HBM),
        scratch_shapes=[pltpu.VMEM((tok_count, width), jnp.bfloat16), pltpu.SemaphoreType.DMA],
        compiler_params=pltpu.CompilerParams(vmem_limit_bytes=8 * 1024 * 1024),
    )(last, partial, w_last)
    return mixed.reshape(seq_count, tok_count, width)


def shards(tokens, norm_gain, w_in, w_out):
    seq_count, tok_count, _ = tokens.shape
    shape = (lax.axis_size("row"), lax.axis_size("col"))
    if seq_count == 1 and fused_fits(*shape, tok_count, w_in.shape[1]):
        return fused_shards(tokens, norm_gain, w_in, w_out)
    return factored_shards(tokens, norm_gain, w_in, w_out)


def solution(mesh):
    return jax.shard_map(
        shards,
        mesh=mesh,
        in_specs=(P("grp", ("row", "col"), None), P(), P(), P()),
        out_specs=P("grp", ("row", "col"), None),
        check_vma=False,
    )
```

```python
import functools
import math

import jax
import jax.numpy as jnp
import numpy as np
from jax import lax
from jax.experimental import pallas as pl
from jax.experimental.pallas import tpu as pltpu
from jax.sharding import PartitionSpec as P

GROUP_CH = 128


TWO_PI = 2.0 * math.pi
NORM_EPS = 1e-06
HIGHEST = lax.Precision.HIGHEST


def phase_tables(rows, cols, period):
    left = lax.broadcasted_iota(jnp.int32, (rows, cols), 0)
    right = lax.broadcasted_iota(jnp.int32, (rows, cols), 1)
    angles = (left * right % period).astype(jnp.float32) * (TWO_PI / period)
    return (jnp.cos(angles), jnp.sin(angles))


def rotate_by(pattern, cos_table, sin_table, real_part, imag_part):

    def apply(table, data):
        return jnp.einsum(pattern, table, data, precision=HIGHEST)

    return (
        apply(cos_table, real_part) + apply(sin_table, imag_part),
        apply(cos_table, imag_part) - apply(sin_table, real_part),
    )


def twist(real_part, imag_part, cos_table, sin_table):
    return (
        real_part * cos_table + imag_part * sin_table,
        imag_part * cos_table - real_part * sin_table,
    )


def factored_shards(tokens, norm_gain, w_in, w_out):
    seq_count, tok_count, width = tokens.shape
    feat_count = w_in.shape[1]
    row_count = lax.axis_size("row")
    col_count = lax.axis_size("col")
    block_len = tok_count * col_count
    length = block_len * row_count
    sub_feats = feat_count // row_count
    fine_count = tok_count // row_count
    item_count = seq_count * feat_count // col_count
    ortho_scale = 1.0 / math.sqrt(length * GROUP_CH)
    widened = tokens.astype(jnp.float32)
    factor = lax.rsqrt(jnp.mean(widened * widened, -1, keepdims=True) + NORM_EPS)
    normed = (widened * factor * norm_gain.astype(jnp.float32)).astype(jnp.bfloat16)
    mixin = jnp.einsum("std,df->sft", normed, w_in, preferred_element_type=jnp.float32).astype(
        jnp.bfloat16
    )
    row_cos, row_sin = phase_tables(row_count, row_count, row_count)
    chan_cos, chan_sin = phase_tables(GROUP_CH, GROUP_CH, GROUP_CH)
    stacked_shape = (seq_count, sub_feats, row_count, tok_count)
    grouped = mixin.astype(jnp.float32).reshape(
        seq_count, feat_count // GROUP_CH, GROUP_CH, tok_count
    )
    spec_real = jnp.einsum("sgqt,qm->sgmt", grouped, chan_cos, precision=HIGHEST).reshape(
        seq_count, feat_count, tok_count
    )
    spec_imag = -jnp.einsum("sgqt,qm->sgmt", grouped, chan_sin, precision=HIGHEST).reshape(
        seq_count, feat_count, tok_count
    )
    arrived = (
        lax.all_to_all(
            spec_real.astype(jnp.bfloat16), "row", split_axis=1, concat_axis=2, tiled=True
        ).astype(spec_real.dtype),
        lax.all_to_all(
            spec_imag.astype(jnp.bfloat16), "row", split_axis=1, concat_axis=2, tiled=True
        ).astype(spec_imag.dtype),
    )
    stacked_real = arrived[0].reshape(stacked_shape)
    stacked_imag = arrived[1].reshape(stacked_shape)
    real_part, imag_part = rotate_by("ka,sfat->skft", row_cos, row_sin, stacked_real, stacked_imag)
    freq_low = lax.broadcasted_iota(jnp.int32, (row_count, tok_count), 0)
    place = lax.axis_index("col") * tok_count + lax.broadcasted_iota(
        jnp.int32, (row_count, tok_count), 1
    )
    angles = (freq_low * place % length).astype(jnp.float32) * (TWO_PI / length)
    real_part, imag_part = twist(
        real_part, imag_part, jnp.cos(angles)[None, :, None, :], jnp.sin(angles)[None, :, None, :]
    )
    sending = (
        real_part.reshape(item_count, col_count, 1, tok_count),
        imag_part.reshape(item_count, col_count, 1, tok_count),
    )
    col_cos, col_sin = phase_tables(col_count, col_count, col_count)
    mid_cos, mid_sin = phase_tables(col_count, tok_count, block_len)
    tok_cos, tok_sin = phase_tables(tok_count, tok_count, tok_count)
    tok_cos = tok_cos.reshape(row_count, fine_count, tok_count)
    tok_sin = tok_sin.reshape(row_count, fine_count, tok_count)
    span_real, span_imag = rotate_by(
        "uc,qct->qut",
        col_cos,
        col_sin,
        lax.all_to_all(
            sending[0].astype(jnp.bfloat16), "col", split_axis=1, concat_axis=2, tiled=True
        ).astype(jnp.float32)[:, 0],
        lax.all_to_all(
            sending[1].astype(jnp.bfloat16), "col", split_axis=1, concat_axis=2, tiled=True
        ).astype(jnp.float32)[:, 0],
    )
    span_real, span_imag = twist(span_real, span_imag, mid_cos, mid_sin)
    span_real, span_imag = rotate_by("rjt,qut->rjuq", tok_cos, tok_sin, span_real, span_imag)
    owner_shape = (row_count, col_count, fine_count, span_real.shape[-1], 1)
    span_real, span_imag = (span_real.reshape(owner_shape), span_imag.reshape(owner_shape))
    rounded = (span_real * ortho_scale).astype(jnp.bfloat16)
    returned = lax.all_to_all(rounded, "col", split_axis=1, concat_axis=4, tiled=True)
    layout = (row_count, fine_count, seq_count, row_count, sub_feats)
    spectrum = lax.all_to_all(
        returned.reshape(layout), "row", split_axis=0, concat_axis=4, tiled=True
    )
    spectrum = spectrum.reshape(fine_count, seq_count, row_count, feat_count)
    mixed = jnp.einsum("jskf,fd->sjkd", spectrum, w_out, preferred_element_type=jnp.float32).astype(
        jnp.bfloat16
    )
    return mixed.reshape(seq_count, fine_count * row_count, width)


CHUNKS = (1, 3)
LATE = 2
LANES = 128
MESH = pl.DeviceIdType.MESH


def host_spots(row_count):
    low, high = row_count // 2 - 1, row_count // 2
    return [(low, 1), (low, 3), (high, 3), (high, 1)]


def fused_fits(row_count, col_count, tok_count, feat_count):
    return (
        row_count == 4
        and col_count == 4
        and tok_count == LANES
        and GROUP_CH == LANES
        and feat_count == GROUP_CH * 4
    )


def row_slots(peers):
    pairs = [(0, peers // 2)] + [(a, peers - a) for a in range(1, peers // 2)]
    return [a for parity in (0, 1) for pair in pairs if pair[0] % 2 == parity for a in pair]


def host_tables(peers, tok_count):
    length = peers * tok_count
    half = GROUP_CH // 2
    q = np.arange(GROUP_CH)[:, None]
    m = np.arange(half)[None, :]
    chan = np.zeros((GROUP_CH, GROUP_CH))
    chan[:, :half] = np.cos(2 * np.pi * (q * m % GROUP_CH) / GROUP_CH)
    chan[:, half:] = -np.sin(2 * np.pi * (q * m % GROUP_CH) / GROUP_CH)
    chan[:, half] = np.cos(np.pi * q[:, 0])
    t = np.arange(tok_count)[None, :]
    b = np.arange(tok_count)[:, None]
    scale = 1.0 / math.sqrt(length * GROUP_CH)
    mid = np.zeros((peers, tok_count, 2, tok_count))
    for a in range(peers):
        angle = 2 * np.pi * (t * (peers * b + a) % length) / length
        mid[a, :, 0] = np.cos(angle) * scale
        mid[a, :, 1] = -np.sin(angle) * scale * (1 if a <= peers // 2 else -1)
    mid = mid.reshape(peers, tok_count, 2 * tok_count)[row_slots(peers)]
    fold = np.zeros((GROUP_CH, GROUP_CH))
    fold[0, 0] = 1
    fold[half, half] = 1
    for a in range(1, half):
        fold[a, a] = 1
        fold[a, GROUP_CH - a] = 1
        fold[half + a, a] = 1
        fold[half + a, GROUP_CH - a] = -1
    return [jnp.asarray(x, jnp.bfloat16) for x in (np.stack([chan, fold]), mid)]


def plus(a, b):
    if a is None or b is None:
        return b if a is None else a
    return a + b


def minus(a, b):
    if a is None or b is None:
        return a if b is None else -b
    return a - b


def times(a, factor):
    return None if a is None else a * factor


def widen(a):
    return None if a is None else a.astype(jnp.float32)


def even_transform(x):
    r = math.sqrt(0.5)
    e = [widen(plus(x[s], x[s + 8])) for s in range(8)]
    p04, n04 = plus(e[0], e[4]), minus(e[0], e[4])
    p26, n26 = plus(e[2], e[6]), minus(e[2], e[6])
    p15, n15 = plus(e[1], e[5]), minus(e[1], e[5])
    p37, n37 = plus(e[3], e[7]), minus(e[3], e[7])
    low, high = plus(p04, p26), plus(p15, p37)
    even_cos = times(minus(n15, n37), r)
    even_sin = times(plus(n15, n37), r)
    return {
        0: (plus(low, high), None),
        8: (minus(low, high), None),
        4: (minus(p04, p26), minus(p15, p37)),
        2: (plus(n04, even_cos), plus(even_sin, n26)),
        6: (minus(n04, even_cos), minus(even_sin, n26)),
    }


def odd_transform(x):
    r = math.sqrt(0.5)
    c1, s1 = math.cos(math.pi / 8), math.sin(math.pi / 8)
    o = [widen(minus(x[s], x[s + 8])) for s in range(8)]
    f1, f2, f3 = minus(o[1], o[7]), times(minus(o[2], o[6]), r), minus(o[3], o[5])
    g1, g2, g3 = plus(o[1], o[7]), times(plus(o[2], o[6]), r), plus(o[3], o[5])
    up, down = plus(o[0], f2), minus(o[0], f2)
    one = plus(times(f1, c1), times(f3, s1))
    two = minus(times(f1, s1), times(f3, c1))
    add, sub = plus(g2, o[4]), minus(g2, o[4])
    three = plus(times(g1, s1), times(g3, c1))
    four = minus(times(g1, c1), times(g3, s1))
    return {
        1: (plus(up, one), plus(three, add)),
        7: (minus(up, one), minus(three, add)),
        3: (plus(down, two), plus(four, sub)),
        5: (minus(down, two), minus(four, sub)),
    }


def fused_kernel(
    shape,
    tokens_hbm,
    gain_hbm,
    w_in_hbm,
    small_hbm,
    mid_hbm,
    w_out_hbm,
    last_ref,
    partial_ref,
    w_last,
    tokens,
    gain,
    w_in,
    small,
    mid,
    w_out,
    w_first,
    natural,
    first_out,
    first_in,
    blocks,
    second_out,
    second_in,
    early,
    load_sem,
    send_sem,
    recv_a,
    recv_b,
):
    row_count, col_count = shape
    peers = row_count * col_count
    tok_count, width = tokens.shape
    feat_count = w_in.shape[1]
    fine = tok_count // peers
    groups = feat_count // GROUP_CH
    half = GROUP_CH // 2
    hosts = [r * col_count + c for r, c in host_spots(row_count)]
    row, col = lax.axis_index("row"), lax.axis_index("col")
    me = row * col_count + col
    is_host = me == hosts[0]
    for spot in hosts[1:]:
        is_host = is_host | (me == spot)

    def device(index):
        return {"row": index // col_count, "col": index % col_count}

    load_tokens = pltpu.make_async_copy(tokens_hbm, tokens, load_sem.at[0])
    load_gain = pltpu.make_async_copy(gain_hbm, gain, load_sem.at[1])
    load_small = pltpu.make_async_copy(small_hbm, small, load_sem.at[2])
    load_mid = pltpu.make_async_copy(mid_hbm, mid, load_sem.at[3])
    load_out = pltpu.make_async_copy(w_out_hbm, w_out, load_sem.at[4])
    edges = [sum(CHUNKS[:c]) for c in range(len(CHUNKS) + 1)]
    spans = [
        (edges[c] * GROUP_CH, (edges[c + 1] - edges[c]) * GROUP_CH) for c in range(len(CHUNKS))
    ]
    load_w = []
    for c, (left, size) in enumerate(spans):
        at = (slice(None), pl.ds(left, size))
        load_w.append(pltpu.make_async_copy(w_in_hbm.at[at], w_in.at[at], load_sem.at[5 + c]))
    load_tokens.start()
    load_gain.start()
    load_w[0].start()
    load_small.start()
    for load in load_w[1:]:
        load.start()

    barrier = pltpu.get_barrier_semaphore()

    @pl.when(is_host)
    def _():
        for step in range(1, peers):
            target = lax.rem(me + step, peers)
            pl.semaphore_signal(
                barrier,
                inc=1,
                device_id={"row": target // col_count, "col": lax.rem(target, col_count)},
                device_id_type=MESH,
            )

    load_tokens.wait()
    load_gain.wait()
    scaled = tokens[...] * gain[...].reshape(1, width)
    widened = tokens[...].astype(jnp.float32)
    factor = lax.rsqrt(jnp.mean(widened * widened, -1, keepdims=True) + NORM_EPS)
    for c, (left, size) in enumerate(spans):
        load_w[c].wait()
        if c == len(spans) - 1:

            @pl.when(is_host)
            def _():
                load_mid.start()

            load_out.start()
        mixin = jnp.dot(
            scaled, w_in[:, left : left + size], preferred_element_type=jnp.float32
        )
        mixin = (mixin * factor).astype(jnp.bfloat16)
        if c == 0:
            load_small.wait()
        for g in range(edges[c], edges[c + 1]):
            at = g * GROUP_CH - left
            first_out[g] = jnp.dot(
                mixin[:, at : at + GROUP_CH], small[0], preferred_element_type=jnp.float32
            ).astype(jnp.bfloat16)
        if c == 0:

            @pl.when(is_host)
            def _():
                pl.semaphore_wait(barrier, groups - 1)

            @pl.when(jnp.logical_not(is_host))
            def _():
                pl.semaphore_wait(barrier, groups)

        for g in range(edges[c], edges[c + 1]):
            spot = hosts[g]

            @pl.when(me != spot)
            def _():
                pltpu.make_async_remote_copy(
                    src_ref=first_out.at[g],
                    dst_ref=first_in.at[me],
                    send_sem=send_sem.at[0],
                    recv_sem=recv_a.at[jnp.where(row == row_count - 1, 1, 0)],
                    device_id=device(spot),
                    device_id_type=MESH,
                ).start()

            @pl.when(me == spot)
            def _():
                first_in[me] = first_out[g]

    load_out.wait()
    for g in range(groups):
        span = slice(g * GROUP_CH, (g + 1) * GROUP_CH)
        folded = jnp.dot(small[1], w_out[span, :], preferred_element_type=jnp.float32)
        if g < groups - LATE:
            w_first[span, :] = folded.astype(jnp.bfloat16)
        else:
            at = (g - groups + LATE) * GROUP_CH
            w_last[at : at + GROUP_CH, :] = folded.astype(jnp.bfloat16)

    slots = row_slots(peers)

    @pl.when(is_host)
    def _():
        load_mid.wait()
        step = 16
        late_count = col_count
        late_top = peers - late_count
        rest = first_in.at[pl.ds(0, late_top - 1)]
        pltpu.make_async_copy(rest, rest, recv_a.at[0]).wait()
        for transform in (even_transform, odd_transform):
            for top in range(0, tok_count, step):
                rows = slice(top, top + step)
                arrived = [first_in[s, rows] for s in range(late_top)] + [None] * late_count
                for a, (cosine, sine) in transform(arrived).items():
                    early[a, 0, rows] = cosine
                    if sine is not None:
                        early[a, 1, rows] = sine
        rest = first_in.at[pl.ds(0, late_count)]
        pltpu.make_async_copy(rest, rest, recv_a.at[1]).wait()
        cosine_lane = lax.broadcasted_iota(jnp.int16, (step, LANES), 1) <= half
        zero = jnp.zeros((step, LANES), jnp.bfloat16)
        for parity, transform in enumerate((even_transform, odd_transform)):
            for top in range(0, tok_count, step):
                rows = slice(top, top + step)
                arrived = [None] * late_top + [first_in[s, rows] for s in range(late_top, peers)]
                for a, (cosine, sine) in transform(arrived).items():
                    cosine = plus(early[a, 0, rows], cosine)
                    sine = None if sine is None else plus(early[a, 1, rows], sine)
                    cosine = cosine.astype(jnp.bfloat16)
                    sine = zero if sine is None else sine.astype(jnp.bfloat16)
                    blocks[a, top : top + step] = jnp.where(cosine_lane, cosine, sine)
                    blocks[a, tok_count + top : tok_count + top + step] = jnp.where(
                        cosine_lane, sine, -cosine
                    )
            for i in range(parity * peers // 2, (parity + 1) * peers // 2, 2):
                pair = [
                    jnp.dot(
                        mid[i + n], blocks[min(a, peers - a)], preferred_element_type=jnp.float32
                    ).reshape(peers, fine, LANES)
                    for n, a in enumerate(slots[i : i + 2])
                ]
                second_out[:, i * fine : (i + 2) * fine, :] = jnp.concatenate(pair, axis=1).astype(
                    jnp.bfloat16
                )

    served = [0, row_count - 1, *range(1, row_count - 1)]
    served = [r * col_count + c for r in served for c in range(col_count)]
    for g, spot in enumerate(hosts):

        @pl.when(me == spot)
        def _():
            for target in served:
                if target != spot:
                    pltpu.make_async_remote_copy(
                        src_ref=second_out.at[target],
                        dst_ref=second_in.at[g],
                        send_sem=send_sem.at[1],
                        recv_sem=recv_b.at[g // LATE],
                        device_id=device(target),
                        device_id_type=MESH,
                    ).start()
            second_in[g] = second_out[spot]

    @pl.when(is_host)
    def _():
        sent = first_out.at[pl.ds(0, groups - 1)]
        pltpu.make_async_copy(sent, sent, send_sem.at[0]).wait()

    @pl.when(jnp.logical_not(is_host))
    def _():
        pltpu.make_async_copy(first_out, first_out, send_sem.at[0]).wait()

    flipped = jnp.where(lax.broadcasted_iota(jnp.int32, (fine, LANES), 1) > half, -1.0, 1.0)

    def arrive(pair):
        own = (me == hosts[pair * LATE]) | (me == hosts[pair * LATE + 1])

        @pl.when(own)
        def _():
            one = second_in.at[pair * LATE]
            pltpu.make_async_copy(one, one, recv_b.at[pair]).wait()

        @pl.when(jnp.logical_not(own))
        def _():
            both = second_in.at[pl.ds(pair * LATE, LATE)]
            pltpu.make_async_copy(both, both, recv_b.at[pair]).wait()

    def collect(g):
        for i, a in enumerate(slots):
            part = second_in[g, i * fine : (i + 1) * fine].astype(jnp.float32)
            if a > peers // 2:
                part = part * flipped
            natural[g, pl.ds(a, fine, stride=peers), :] = part
        return natural[g].astype(jnp.bfloat16)

    arrive(0)
    values = [collect(g) for g in range(LATE)]
    partial_ref[...] = jnp.dot(
        jnp.concatenate(values, axis=1), w_first[...], preferred_element_type=jnp.float32
    )
    arrive(1)
    for g in range(LATE):
        last_ref[:, g * GROUP_CH : (g + 1) * GROUP_CH] = collect(LATE + g)

    @pl.when(is_host)
    def _():
        sent = second_out.at[pl.ds(0, peers - 1)]
        pltpu.make_async_copy(sent, sent, send_sem.at[1]).wait()


def project_kernel(chunks, last, partial, w_last, out_hbm, staged, sem):
    size = w_last.shape[1] // chunks
    for i in range(chunks):
        lanes = slice(i * size, (i + 1) * size)
        staged[:, lanes] = (
            partial[:, lanes]
            + jnp.dot(last[...], w_last[:, lanes], preferred_element_type=jnp.float32)
        ).astype(staged.dtype)
        span = pl.ds(i * size, size)
        pltpu.make_async_copy(staged.at[:, span], out_hbm.at[:, span], sem).start()
    pltpu.make_async_copy(staged, out_hbm, sem).wait()


def fused_shards(tokens, norm_gain, w_in, w_out):
    seq_count, tok_count, width = tokens.shape
    feat_count = w_in.shape[1]
    shape = (lax.axis_size("row"), lax.axis_size("col"))
    peers = shape[0] * shape[1]
    groups = feat_count // GROUP_CH
    tables = host_tables(peers, tok_count)
    operands = [tokens.reshape(tok_count, width), norm_gain, w_in, *tables, w_out]
    held = [pltpu.VMEM(x.shape, x.dtype) for x in operands]
    last, partial, w_last = pl.pallas_call(
        functools.partial(fused_kernel, shape),
        out_shape=(
            pltpu.VMEM((tok_count, LATE * GROUP_CH), jnp.bfloat16),
            pltpu.VMEM((tok_count, width), jnp.float32),
            pltpu.VMEM((LATE * GROUP_CH, width), jnp.bfloat16),
        ),
        in_specs=[pl.BlockSpec(memory_space=pltpu.HBM)] * len(operands),
        out_specs=(pl.BlockSpec(memory_space=pltpu.VMEM),) * 3,
        scratch_shapes=held
        + [
            pltpu.VMEM((feat_count - LATE * GROUP_CH, width), jnp.bfloat16),
            pltpu.VMEM((groups, tok_count, GROUP_CH), jnp.float32),
            pltpu.VMEM((groups, tok_count, GROUP_CH), jnp.bfloat16),
            pltpu.VMEM((peers, tok_count, GROUP_CH), jnp.bfloat16),
            pltpu.VMEM((peers // 2 + 1, 2 * tok_count, GROUP_CH), jnp.bfloat16),
            pltpu.VMEM((peers, tok_count, GROUP_CH), jnp.bfloat16),
            pltpu.VMEM((groups, tok_count, GROUP_CH), jnp.bfloat16),
            pltpu.VMEM((peers // 2 + 1, 2, tok_count, GROUP_CH), jnp.float32),
            pltpu.SemaphoreType.DMA((5 + len(CHUNKS),)),
            pltpu.SemaphoreType.DMA((2,)),
            pltpu.SemaphoreType.DMA((2,)),
            pltpu.SemaphoreType.DMA((groups // LATE,)),
        ],
        compiler_params=pltpu.CompilerParams(
            collective_id=0, has_side_effects=True, vmem_limit_bytes=62_000_000
        ),
    )(*operands)
    pieces = max(1, width // 512)
    mixed = pl.pallas_call(
        functools.partial(project_kernel, pieces),
        out_shape=jax.ShapeDtypeStruct((tok_count, width), jnp.bfloat16),
        in_specs=[pl.BlockSpec(memory_space=pltpu.VMEM)] * 3,
        out_specs=pl.BlockSpec(memory_space=pltpu.HBM),
        scratch_shapes=[pltpu.VMEM((tok_count, width), jnp.bfloat16), pltpu.SemaphoreType.DMA],
        compiler_params=pltpu.CompilerParams(vmem_limit_bytes=8 * 1024 * 1024),
    )(last, partial, w_last)
    return mixed.reshape(seq_count, tok_count, width)


def shards(tokens, norm_gain, w_in, w_out):
    seq_count, tok_count, _ = tokens.shape
    shape = (lax.axis_size("row"), lax.axis_size("col"))
    if seq_count == 1 and fused_fits(*shape, tok_count, w_in.shape[1]):
        return fused_shards(tokens, norm_gain, w_in, w_out)
    return factored_shards(tokens, norm_gain, w_in, w_out)


def solution(mesh):
    return jax.shard_map(
        shards,
        mesh=mesh,
        in_specs=(P("grp", ("row", "col"), None), P(), P(), P()),
        out_specs=P("grp", ("row", "col"), None),
        check_vma=False,
    )
```

```python
import functools
import math

import jax
import jax.numpy as jnp
import numpy as np
from jax import lax
from jax.experimental import pallas as pl
from jax.experimental.pallas import tpu as pltpu
from jax.sharding import PartitionSpec as P

GROUP_CH = 128


TWO_PI = 2.0 * math.pi
NORM_EPS = 1e-06
HIGHEST = lax.Precision.HIGHEST


def phase_tables(rows, cols, period):
    left = lax.broadcasted_iota(jnp.int32, (rows, cols), 0)
    right = lax.broadcasted_iota(jnp.int32, (rows, cols), 1)
    angles = (left * right % period).astype(jnp.float32) * (TWO_PI / period)
    return (jnp.cos(angles), jnp.sin(angles))


def rotate_by(pattern, cos_table, sin_table, real_part, imag_part):

    def apply(table, data):
        return jnp.einsum(pattern, table, data, precision=HIGHEST)

    return (
        apply(cos_table, real_part) + apply(sin_table, imag_part),
        apply(cos_table, imag_part) - apply(sin_table, real_part),
    )


def twist(real_part, imag_part, cos_table, sin_table):
    return (
        real_part * cos_table + imag_part * sin_table,
        imag_part * cos_table - real_part * sin_table,
    )


def factored_shards(tokens, norm_gain, w_in, w_out):
    seq_count, tok_count, width = tokens.shape
    feat_count = w_in.shape[1]
    row_count = lax.axis_size("row")
    col_count = lax.axis_size("col")
    block_len = tok_count * col_count
    length = block_len * row_count
    sub_feats = feat_count // row_count
    fine_count = tok_count // row_count
    item_count = seq_count * feat_count // col_count
    ortho_scale = 1.0 / math.sqrt(length * GROUP_CH)
    widened = tokens.astype(jnp.float32)
    factor = lax.rsqrt(jnp.mean(widened * widened, -1, keepdims=True) + NORM_EPS)
    normed = (widened * factor * norm_gain.astype(jnp.float32)).astype(jnp.bfloat16)
    mixin = jnp.einsum("std,df->sft", normed, w_in, preferred_element_type=jnp.float32).astype(
        jnp.bfloat16
    )
    row_cos, row_sin = phase_tables(row_count, row_count, row_count)
    chan_cos, chan_sin = phase_tables(GROUP_CH, GROUP_CH, GROUP_CH)
    stacked_shape = (seq_count, sub_feats, row_count, tok_count)
    grouped = mixin.astype(jnp.float32).reshape(
        seq_count, feat_count // GROUP_CH, GROUP_CH, tok_count
    )
    spec_real = jnp.einsum("sgqt,qm->sgmt", grouped, chan_cos, precision=HIGHEST).reshape(
        seq_count, feat_count, tok_count
    )
    spec_imag = -jnp.einsum("sgqt,qm->sgmt", grouped, chan_sin, precision=HIGHEST).reshape(
        seq_count, feat_count, tok_count
    )
    arrived = (
        lax.all_to_all(
            spec_real.astype(jnp.bfloat16), "row", split_axis=1, concat_axis=2, tiled=True
        ).astype(spec_real.dtype),
        lax.all_to_all(
            spec_imag.astype(jnp.bfloat16), "row", split_axis=1, concat_axis=2, tiled=True
        ).astype(spec_imag.dtype),
    )
    stacked_real = arrived[0].reshape(stacked_shape)
    stacked_imag = arrived[1].reshape(stacked_shape)
    real_part, imag_part = rotate_by("ka,sfat->skft", row_cos, row_sin, stacked_real, stacked_imag)
    freq_low = lax.broadcasted_iota(jnp.int32, (row_count, tok_count), 0)
    place = lax.axis_index("col") * tok_count + lax.broadcasted_iota(
        jnp.int32, (row_count, tok_count), 1
    )
    angles = (freq_low * place % length).astype(jnp.float32) * (TWO_PI / length)
    real_part, imag_part = twist(
        real_part, imag_part, jnp.cos(angles)[None, :, None, :], jnp.sin(angles)[None, :, None, :]
    )
    sending = (
        real_part.reshape(item_count, col_count, 1, tok_count),
        imag_part.reshape(item_count, col_count, 1, tok_count),
    )
    col_cos, col_sin = phase_tables(col_count, col_count, col_count)
    mid_cos, mid_sin = phase_tables(col_count, tok_count, block_len)
    tok_cos, tok_sin = phase_tables(tok_count, tok_count, tok_count)
    tok_cos = tok_cos.reshape(row_count, fine_count, tok_count)
    tok_sin = tok_sin.reshape(row_count, fine_count, tok_count)
    span_real, span_imag = rotate_by(
        "uc,qct->qut",
        col_cos,
        col_sin,
        lax.all_to_all(
            sending[0].astype(jnp.bfloat16), "col", split_axis=1, concat_axis=2, tiled=True
        ).astype(jnp.float32)[:, 0],
        lax.all_to_all(
            sending[1].astype(jnp.bfloat16), "col", split_axis=1, concat_axis=2, tiled=True
        ).astype(jnp.float32)[:, 0],
    )
    span_real, span_imag = twist(span_real, span_imag, mid_cos, mid_sin)
    span_real, span_imag = rotate_by("rjt,qut->rjuq", tok_cos, tok_sin, span_real, span_imag)
    owner_shape = (row_count, col_count, fine_count, span_real.shape[-1], 1)
    span_real, span_imag = (span_real.reshape(owner_shape), span_imag.reshape(owner_shape))
    rounded = (span_real * ortho_scale).astype(jnp.bfloat16)
    returned = lax.all_to_all(rounded, "col", split_axis=1, concat_axis=4, tiled=True)
    layout = (row_count, fine_count, seq_count, row_count, sub_feats)
    spectrum = lax.all_to_all(
        returned.reshape(layout), "row", split_axis=0, concat_axis=4, tiled=True
    )
    spectrum = spectrum.reshape(fine_count, seq_count, row_count, feat_count)
    mixed = jnp.einsum("jskf,fd->sjkd", spectrum, w_out, preferred_element_type=jnp.float32).astype(
        jnp.bfloat16
    )
    return mixed.reshape(seq_count, fine_count * row_count, width)


CHUNKS = (1, 3)
LATE = 2
LANES = 128
MESH = pl.DeviceIdType.MESH


def host_spots(row_count):
    low, high = row_count // 2 - 1, row_count // 2
    return [(low, 1), (low, 3), (high, 3), (high, 1)]


def fused_fits(row_count, col_count, tok_count, feat_count):
    return (
        row_count == 4
        and col_count == 4
        and tok_count == LANES
        and GROUP_CH == LANES
        and feat_count == GROUP_CH * 4
    )


def row_slots(peers):
    pairs = [(0, peers // 2)] + [(a, peers - a) for a in range(1, peers // 2)]
    return [a for parity in (0, 1) for pair in pairs if pair[0] % 2 == parity for a in pair]


def host_tables(peers, tok_count):
    length = peers * tok_count
    half = GROUP_CH // 2
    q = np.arange(GROUP_CH)[:, None]
    m = np.arange(half)[None, :]
    chan = np.zeros((GROUP_CH, GROUP_CH))
    chan[:, :half] = np.cos(2 * np.pi * (q * m % GROUP_CH) / GROUP_CH)
    chan[:, half:] = -np.sin(2 * np.pi * (q * m % GROUP_CH) / GROUP_CH)
    chan[:, half] = np.cos(np.pi * q[:, 0])
    t = np.arange(tok_count)[None, :]
    b = np.arange(tok_count)[:, None]
    scale = 1.0 / math.sqrt(length * GROUP_CH)
    mid = np.zeros((peers, tok_count, 2, tok_count))
    for a in range(peers):
        angle = 2 * np.pi * (t * (peers * b + a) % length) / length
        mid[a, :, 0] = np.cos(angle) * scale
        mid[a, :, 1] = -np.sin(angle) * scale * (1 if a <= peers // 2 else -1)
    mid = mid.reshape(peers, tok_count, 2 * tok_count)[row_slots(peers)]
    fold = np.zeros((GROUP_CH, GROUP_CH))
    fold[0, 0] = 1
    fold[half, half] = 1
    for a in range(1, half):
        fold[a, a] = 1
        fold[a, GROUP_CH - a] = 1
        fold[half + a, a] = 1
        fold[half + a, GROUP_CH - a] = -1
    return [jnp.asarray(x, jnp.bfloat16) for x in (np.stack([chan, fold]), mid)]


def plus(a, b):
    if a is None or b is None:
        return b if a is None else a
    return a + b


def minus(a, b):
    if a is None or b is None:
        return a if b is None else -b
    return a - b


def times(a, factor):
    return None if a is None else a * factor


def widen(a):
    return None if a is None else a.astype(jnp.float32)


def even_transform(x):
    r = math.sqrt(0.5)
    e = [widen(plus(x[s], x[s + 8])) for s in range(8)]
    p04, n04 = plus(e[0], e[4]), minus(e[0], e[4])
    p26, n26 = plus(e[2], e[6]), minus(e[2], e[6])
    p15, n15 = plus(e[1], e[5]), minus(e[1], e[5])
    p37, n37 = plus(e[3], e[7]), minus(e[3], e[7])
    low, high = plus(p04, p26), plus(p15, p37)
    even_cos = times(minus(n15, n37), r)
    even_sin = times(plus(n15, n37), r)
    return {
        0: (plus(low, high), None),
        8: (minus(low, high), None),
        4: (minus(p04, p26), minus(p15, p37)),
        2: (plus(n04, even_cos), plus(even_sin, n26)),
        6: (minus(n04, even_cos), minus(even_sin, n26)),
    }


def odd_transform(x):
    r = math.sqrt(0.5)
    c1, s1 = math.cos(math.pi / 8), math.sin(math.pi / 8)
    o = [widen(minus(x[s], x[s + 8])) for s in range(8)]
    f1, f2, f3 = minus(o[1], o[7]), times(minus(o[2], o[6]), r), minus(o[3], o[5])
    g1, g2, g3 = plus(o[1], o[7]), times(plus(o[2], o[6]), r), plus(o[3], o[5])
    up, down = plus(o[0], f2), minus(o[0], f2)
    one = plus(times(f1, c1), times(f3, s1))
    two = minus(times(f1, s1), times(f3, c1))
    add, sub = plus(g2, o[4]), minus(g2, o[4])
    three = plus(times(g1, s1), times(g3, c1))
    four = minus(times(g1, c1), times(g3, s1))
    return {
        1: (plus(up, one), plus(three, add)),
        7: (minus(up, one), minus(three, add)),
        3: (plus(down, two), plus(four, sub)),
        5: (minus(down, two), minus(four, sub)),
    }


def fused_kernel(
    shape,
    tokens_hbm,
    gain_hbm,
    w_in_hbm,
    small_hbm,
    mid_hbm,
    w_out_hbm,
    last_ref,
    partial_ref,
    w_last,
    tokens,
    gain,
    w_in,
    small,
    mid,
    w_out,
    w_first,
    natural,
    first_out,
    first_in,
    blocks,
    second_out,
    second_in,
    early,
    load_sem,
    send_sem,
    recv_a,
    recv_b,
):
    row_count, col_count = shape
    peers = row_count * col_count
    tok_count, width = tokens.shape
    feat_count = w_in.shape[1]
    fine = tok_count // peers
    groups = feat_count // GROUP_CH
    half = GROUP_CH // 2
    hosts = [r * col_count + c for r, c in host_spots(row_count)]
    row, col = lax.axis_index("row"), lax.axis_index("col")
    me = row * col_count + col
    is_host = me == hosts[0]
    group = jnp.int32(0)
    for g in range(1, groups):
        is_host = is_host | (me == hosts[g])
        group = group + jnp.where(me == hosts[g], g, 0)

    def device(index):
        return {"row": index // col_count, "col": index % col_count}

    load_tokens = pltpu.make_async_copy(tokens_hbm, tokens, load_sem.at[0])
    load_gain = pltpu.make_async_copy(gain_hbm, gain, load_sem.at[1])
    load_small = pltpu.make_async_copy(small_hbm, small, load_sem.at[2])
    load_mid = pltpu.make_async_copy(mid_hbm, mid, load_sem.at[3])
    load_out = pltpu.make_async_copy(w_out_hbm, w_out, load_sem.at[4])
    edges = [sum(CHUNKS[:c]) for c in range(len(CHUNKS) + 1)]
    spans = [
        (edges[c] * GROUP_CH, (edges[c + 1] - edges[c]) * GROUP_CH) for c in range(len(CHUNKS))
    ]
    load_w = []
    for c, (left, size) in enumerate(spans):
        at = (slice(None), pl.ds(left, size))
        load_w.append(pltpu.make_async_copy(w_in_hbm.at[at], w_in.at[at], load_sem.at[5 + c]))
    load_tokens.start()
    load_gain.start()
    load_w[0].start()
    load_small.start()
    for load in load_w[1:]:
        load.start()

    barrier = pltpu.get_barrier_semaphore()

    @pl.when(is_host)
    def _():
        for step in range(1, peers):
            target = lax.rem(me + step, peers)
            pl.semaphore_signal(
                barrier,
                inc=1,
                device_id={"row": target // col_count, "col": lax.rem(target, col_count)},
                device_id_type=MESH,
            )

    load_tokens.wait()
    load_gain.wait()
    scaled = tokens[...] * gain[...].reshape(1, width)
    widened = tokens[...].astype(jnp.float32)
    factor = lax.rsqrt(jnp.mean(widened * widened, -1, keepdims=True) + NORM_EPS)
    for c, (left, size) in enumerate(spans):
        load_w[c].wait()
        if c == len(spans) - 1:

            @pl.when(is_host)
            def _():
                load_mid.start()

            load_out.start()
        mixin = jnp.dot(
            scaled, w_in[:, left : left + size], preferred_element_type=jnp.float32
        )
        mixin = (mixin * factor).astype(jnp.bfloat16)
        if c == 0:
            load_small.wait()
        for g in range(edges[c], edges[c + 1]):
            at = g * GROUP_CH - left
            first_out[g] = jnp.dot(
                mixin[:, at : at + GROUP_CH], small[0], preferred_element_type=jnp.float32
            ).astype(jnp.bfloat16)
        if c == 0:

            @pl.when(is_host)
            def _():
                pl.semaphore_wait(barrier, groups - 1)

            @pl.when(jnp.logical_not(is_host))
            def _():
                pl.semaphore_wait(barrier, groups)

        for g in range(edges[c], edges[c + 1]):
            spot = hosts[g]

            @pl.when(me != spot)
            def _():
                pltpu.make_async_remote_copy(
                    src_ref=first_out.at[g],
                    dst_ref=first_in.at[me],
                    send_sem=send_sem.at[0],
                    recv_sem=recv_a.at[jnp.where(row == row_count - 1, 1, 0)],
                    device_id=device(spot),
                    device_id_type=MESH,
                ).start()

            @pl.when(me == spot)
            def _():
                first_in[me] = first_out[g]

    load_out.wait()
    for g in range(groups):
        span = slice(g * GROUP_CH, (g + 1) * GROUP_CH)
        folded = jnp.dot(small[1], w_out[span, :], preferred_element_type=jnp.float32)
        if g < groups - LATE:
            w_first[span, :] = folded.astype(jnp.bfloat16)
        else:
            at = (g - groups + LATE) * GROUP_CH
            w_last[at : at + GROUP_CH, :] = folded.astype(jnp.bfloat16)

    slots = row_slots(peers)

    @pl.when(is_host)
    def _():
        load_mid.wait()
        step = 16
        late_count = col_count
        late_top = peers - late_count
        rest = first_in.at[pl.ds(0, late_top - 1)]
        pltpu.make_async_copy(rest, rest, recv_a.at[0]).wait()
        for transform in (even_transform, odd_transform):
            for top in range(0, tok_count, step):
                rows = slice(top, top + step)
                arrived = [first_in[s, rows] for s in range(late_top)] + [None] * late_count
                for a, (cosine, sine) in transform(arrived).items():
                    early[a, 0, rows] = cosine
                    if sine is not None:
                        early[a, 1, rows] = sine
        rest = first_in.at[pl.ds(0, late_count)]
        pltpu.make_async_copy(rest, rest, recv_a.at[1]).wait()
        cosine_lane = lax.broadcasted_iota(jnp.int16, (step, LANES), 1) <= half
        zero = jnp.zeros((step, LANES), jnp.bfloat16)
        for parity, transform in enumerate((even_transform, odd_transform)):
            for top in range(0, tok_count, step):
                rows = slice(top, top + step)
                arrived = [None] * late_top + [first_in[s, rows] for s in range(late_top, peers)]
                for a, (cosine, sine) in transform(arrived).items():
                    cosine = plus(early[a, 0, rows], cosine)
                    sine = None if sine is None else plus(early[a, 1, rows], sine)
                    cosine = cosine.astype(jnp.bfloat16)
                    sine = zero if sine is None else sine.astype(jnp.bfloat16)
                    blocks[a, top : top + step] = jnp.where(cosine_lane, cosine, sine)
                    blocks[a, tok_count + top : tok_count + top + step] = jnp.where(
                        cosine_lane, sine, -cosine
                    )
            cuts = (0, peers) if parity == 0 else (0, col_count, peers)
            for first, stop in zip(cuts, cuts[1:]):
                for i in range(parity * peers // 2, (parity + 1) * peers // 2, 2):
                    pair = [
                        jnp.dot(
                            mid[i + n, first * fine : stop * fine],
                            blocks[min(a, peers - a)],
                            preferred_element_type=jnp.float32,
                        ).reshape(stop - first, fine, LANES)
                        for n, a in enumerate(slots[i : i + 2])
                    ]
                    second_out[first:stop, i * fine : (i + 2) * fine, :] = jnp.concatenate(
                        pair, axis=1
                    ).astype(jnp.bfloat16)
                if stop == col_count:
                    for target in range(col_count):
                        pltpu.make_async_remote_copy(
                            src_ref=second_out.at[target],
                            dst_ref=second_in.at[group],
                            send_sem=send_sem.at[1],
                            recv_sem=recv_b.at[group // LATE],
                            device_id=device(target),
                            device_id_type=MESH,
                        ).start()

    served = [row_count - 1, *range(1, row_count - 1)]
    served = [r * col_count + c for r in served for c in range(col_count)]
    for g, spot in enumerate(hosts):

        @pl.when(me == spot)
        def _():
            for target in served:
                if target != spot:
                    pltpu.make_async_remote_copy(
                        src_ref=second_out.at[target],
                        dst_ref=second_in.at[g],
                        send_sem=send_sem.at[1],
                        recv_sem=recv_b.at[g // LATE],
                        device_id=device(target),
                        device_id_type=MESH,
                    ).start()
            second_in[g] = second_out[spot]

    @pl.when(is_host)
    def _():
        sent = first_out.at[pl.ds(0, groups - 1)]
        pltpu.make_async_copy(sent, sent, send_sem.at[0]).wait()

    @pl.when(jnp.logical_not(is_host))
    def _():
        pltpu.make_async_copy(first_out, first_out, send_sem.at[0]).wait()

    flipped = jnp.where(lax.broadcasted_iota(jnp.int32, (fine, LANES), 1) > half, -1.0, 1.0)

    def arrive(pair):
        own = (me == hosts[pair * LATE]) | (me == hosts[pair * LATE + 1])

        @pl.when(own)
        def _():
            one = second_in.at[pair * LATE]
            pltpu.make_async_copy(one, one, recv_b.at[pair]).wait()

        @pl.when(jnp.logical_not(own))
        def _():
            both = second_in.at[pl.ds(pair * LATE, LATE)]
            pltpu.make_async_copy(both, both, recv_b.at[pair]).wait()

    def collect(g):
        for i, a in enumerate(slots):
            part = second_in[g, i * fine : (i + 1) * fine].astype(jnp.float32)
            if a > peers // 2:
                part = part * flipped
            natural[g, pl.ds(a, fine, stride=peers), :] = part
        return natural[g].astype(jnp.bfloat16)

    arrive(0)
    values = [collect(g) for g in range(LATE)]
    partial_ref[...] = jnp.dot(
        jnp.concatenate(values, axis=1), w_first[...], preferred_element_type=jnp.float32
    )
    arrive(1)
    for g in range(LATE):
        last_ref[:, g * GROUP_CH : (g + 1) * GROUP_CH] = collect(LATE + g)

    @pl.when(is_host)
    def _():
        sent = second_out.at[pl.ds(0, peers - 1)]
        pltpu.make_async_copy(sent, sent, send_sem.at[1]).wait()


def project_kernel(chunks, last, partial, w_last, out_hbm, staged, sem):
    size = w_last.shape[1] // chunks
    for i in range(chunks):
        lanes = slice(i * size, (i + 1) * size)
        staged[:, lanes] = (
            partial[:, lanes]
            + jnp.dot(last[...], w_last[:, lanes], preferred_element_type=jnp.float32)
        ).astype(staged.dtype)
        span = pl.ds(i * size, size)
        pltpu.make_async_copy(staged.at[:, span], out_hbm.at[:, span], sem).start()
    pltpu.make_async_copy(staged, out_hbm, sem).wait()


def fused_shards(tokens, norm_gain, w_in, w_out):
    seq_count, tok_count, width = tokens.shape
    feat_count = w_in.shape[1]
    shape = (lax.axis_size("row"), lax.axis_size("col"))
    peers = shape[0] * shape[1]
    groups = feat_count // GROUP_CH
    tables = host_tables(peers, tok_count)
    operands = [tokens.reshape(tok_count, width), norm_gain, w_in, *tables, w_out]
    held = [pltpu.VMEM(x.shape, x.dtype) for x in operands]
    last, partial, w_last = pl.pallas_call(
        functools.partial(fused_kernel, shape),
        out_shape=(
            pltpu.VMEM((tok_count, LATE * GROUP_CH), jnp.bfloat16),
            pltpu.VMEM((tok_count, width), jnp.float32),
            pltpu.VMEM((LATE * GROUP_CH, width), jnp.bfloat16),
        ),
        in_specs=[pl.BlockSpec(memory_space=pltpu.HBM)] * len(operands),
        out_specs=(pl.BlockSpec(memory_space=pltpu.VMEM),) * 3,
        scratch_shapes=held
        + [
            pltpu.VMEM((feat_count - LATE * GROUP_CH, width), jnp.bfloat16),
            pltpu.VMEM((groups, tok_count, GROUP_CH), jnp.float32),
            pltpu.VMEM((groups, tok_count, GROUP_CH), jnp.bfloat16),
            pltpu.VMEM((peers, tok_count, GROUP_CH), jnp.bfloat16),
            pltpu.VMEM((peers // 2 + 1, 2 * tok_count, GROUP_CH), jnp.bfloat16),
            pltpu.VMEM((peers, tok_count, GROUP_CH), jnp.bfloat16),
            pltpu.VMEM((groups, tok_count, GROUP_CH), jnp.bfloat16),
            pltpu.VMEM((peers // 2 + 1, 2, tok_count, GROUP_CH), jnp.float32),
            pltpu.SemaphoreType.DMA((5 + len(CHUNKS),)),
            pltpu.SemaphoreType.DMA((2,)),
            pltpu.SemaphoreType.DMA((2,)),
            pltpu.SemaphoreType.DMA((groups // LATE,)),
        ],
        compiler_params=pltpu.CompilerParams(
            collective_id=0, has_side_effects=True, vmem_limit_bytes=62_000_000
        ),
    )(*operands)
    pieces = max(1, width // 512)
    mixed = pl.pallas_call(
        functools.partial(project_kernel, pieces),
        out_shape=jax.ShapeDtypeStruct((tok_count, width), jnp.bfloat16),
        in_specs=[pl.BlockSpec(memory_space=pltpu.VMEM)] * 3,
        out_specs=pl.BlockSpec(memory_space=pltpu.HBM),
        scratch_shapes=[pltpu.VMEM((tok_count, width), jnp.bfloat16), pltpu.SemaphoreType.DMA],
        compiler_params=pltpu.CompilerParams(vmem_limit_bytes=8 * 1024 * 1024),
    )(last, partial, w_last)
    return mixed.reshape(seq_count, tok_count, width)


def shards(tokens, norm_gain, w_in, w_out):
    seq_count, tok_count, _ = tokens.shape
    shape = (lax.axis_size("row"), lax.axis_size("col"))
    if seq_count == 1 and fused_fits(*shape, tok_count, w_in.shape[1]):
        return fused_shards(tokens, norm_gain, w_in, w_out)
    return factored_shards(tokens, norm_gain, w_in, w_out)


def solution(mesh):
    return jax.shard_map(
        shards,
        mesh=mesh,
        in_specs=(P("grp", ("row", "col"), None), P(), P(), P()),
        out_specs=P("grp", ("row", "col"), None),
        check_vma=False,
    )
```

```python
import functools
import math

import jax
import jax.numpy as jnp
import numpy as np
from jax import lax
from jax.experimental import pallas as pl
from jax.experimental.pallas import tpu as pltpu
from jax.sharding import PartitionSpec as P

GROUP_CH = 128


TWO_PI = 2.0 * math.pi
NORM_EPS = 1e-06
HIGHEST = lax.Precision.HIGHEST


def phase_tables(rows, cols, period):
    left = lax.broadcasted_iota(jnp.int32, (rows, cols), 0)
    right = lax.broadcasted_iota(jnp.int32, (rows, cols), 1)
    angles = (left * right % period).astype(jnp.float32) * (TWO_PI / period)
    return (jnp.cos(angles), jnp.sin(angles))


def rotate_by(pattern, cos_table, sin_table, real_part, imag_part):

    def apply(table, data):
        return jnp.einsum(pattern, table, data, precision=HIGHEST)

    return (
        apply(cos_table, real_part) + apply(sin_table, imag_part),
        apply(cos_table, imag_part) - apply(sin_table, real_part),
    )


def twist(real_part, imag_part, cos_table, sin_table):
    return (
        real_part * cos_table + imag_part * sin_table,
        imag_part * cos_table - real_part * sin_table,
    )


def factored_shards(tokens, norm_gain, w_in, w_out):
    seq_count, tok_count, width = tokens.shape
    feat_count = w_in.shape[1]
    row_count = lax.axis_size("row")
    col_count = lax.axis_size("col")
    block_len = tok_count * col_count
    length = block_len * row_count
    sub_feats = feat_count // row_count
    fine_count = tok_count // row_count
    item_count = seq_count * feat_count // col_count
    ortho_scale = 1.0 / math.sqrt(length * GROUP_CH)
    widened = tokens.astype(jnp.float32)
    factor = lax.rsqrt(jnp.mean(widened * widened, -1, keepdims=True) + NORM_EPS)
    normed = (widened * factor * norm_gain.astype(jnp.float32)).astype(jnp.bfloat16)
    mixin = jnp.einsum("std,df->sft", normed, w_in, preferred_element_type=jnp.float32).astype(
        jnp.bfloat16
    )
    row_cos, row_sin = phase_tables(row_count, row_count, row_count)
    chan_cos, chan_sin = phase_tables(GROUP_CH, GROUP_CH, GROUP_CH)
    stacked_shape = (seq_count, sub_feats, row_count, tok_count)
    grouped = mixin.astype(jnp.float32).reshape(
        seq_count, feat_count // GROUP_CH, GROUP_CH, tok_count
    )
    spec_real = jnp.einsum("sgqt,qm->sgmt", grouped, chan_cos, precision=HIGHEST).reshape(
        seq_count, feat_count, tok_count
    )
    spec_imag = -jnp.einsum("sgqt,qm->sgmt", grouped, chan_sin, precision=HIGHEST).reshape(
        seq_count, feat_count, tok_count
    )
    arrived = (
        lax.all_to_all(
            spec_real.astype(jnp.bfloat16), "row", split_axis=1, concat_axis=2, tiled=True
        ).astype(spec_real.dtype),
        lax.all_to_all(
            spec_imag.astype(jnp.bfloat16), "row", split_axis=1, concat_axis=2, tiled=True
        ).astype(spec_imag.dtype),
    )
    stacked_real = arrived[0].reshape(stacked_shape)
    stacked_imag = arrived[1].reshape(stacked_shape)
    real_part, imag_part = rotate_by("ka,sfat->skft", row_cos, row_sin, stacked_real, stacked_imag)
    freq_low = lax.broadcasted_iota(jnp.int32, (row_count, tok_count), 0)
    place = lax.axis_index("col") * tok_count + lax.broadcasted_iota(
        jnp.int32, (row_count, tok_count), 1
    )
    angles = (freq_low * place % length).astype(jnp.float32) * (TWO_PI / length)
    real_part, imag_part = twist(
        real_part, imag_part, jnp.cos(angles)[None, :, None, :], jnp.sin(angles)[None, :, None, :]
    )
    sending = (
        real_part.reshape(item_count, col_count, 1, tok_count),
        imag_part.reshape(item_count, col_count, 1, tok_count),
    )
    col_cos, col_sin = phase_tables(col_count, col_count, col_count)
    mid_cos, mid_sin = phase_tables(col_count, tok_count, block_len)
    tok_cos, tok_sin = phase_tables(tok_count, tok_count, tok_count)
    tok_cos = tok_cos.reshape(row_count, fine_count, tok_count)
    tok_sin = tok_sin.reshape(row_count, fine_count, tok_count)
    span_real, span_imag = rotate_by(
        "uc,qct->qut",
        col_cos,
        col_sin,
        lax.all_to_all(
            sending[0].astype(jnp.bfloat16), "col", split_axis=1, concat_axis=2, tiled=True
        ).astype(jnp.float32)[:, 0],
        lax.all_to_all(
            sending[1].astype(jnp.bfloat16), "col", split_axis=1, concat_axis=2, tiled=True
        ).astype(jnp.float32)[:, 0],
    )
    span_real, span_imag = twist(span_real, span_imag, mid_cos, mid_sin)
    span_real, span_imag = rotate_by("rjt,qut->rjuq", tok_cos, tok_sin, span_real, span_imag)
    owner_shape = (row_count, col_count, fine_count, span_real.shape[-1], 1)
    span_real, span_imag = (span_real.reshape(owner_shape), span_imag.reshape(owner_shape))
    rounded = (span_real * ortho_scale).astype(jnp.bfloat16)
    returned = lax.all_to_all(rounded, "col", split_axis=1, concat_axis=4, tiled=True)
    layout = (row_count, fine_count, seq_count, row_count, sub_feats)
    spectrum = lax.all_to_all(
        returned.reshape(layout), "row", split_axis=0, concat_axis=4, tiled=True
    )
    spectrum = spectrum.reshape(fine_count, seq_count, row_count, feat_count)
    mixed = jnp.einsum("jskf,fd->sjkd", spectrum, w_out, preferred_element_type=jnp.float32).astype(
        jnp.bfloat16
    )
    return mixed.reshape(seq_count, fine_count * row_count, width)


CHUNKS = (1, 3)
LATE = 2
LANES = 128
MESH = pl.DeviceIdType.MESH


def host_spots(row_count):
    low, high = row_count // 2 - 1, row_count // 2
    return [(low, 1), (low, 3), (high, 3), (high, 1)]


def fused_fits(row_count, col_count, tok_count, feat_count):
    return (
        row_count == 4
        and col_count == 4
        and tok_count == LANES
        and GROUP_CH == LANES
        and feat_count == GROUP_CH * 4
    )


def row_slots(peers):
    pairs = [(0, peers // 2)] + [(a, peers - a) for a in range(1, peers // 2)]
    return [a for parity in (0, 1) for pair in pairs if pair[0] % 2 == parity for a in pair]


def host_tables(peers, tok_count):
    length = peers * tok_count
    half = GROUP_CH // 2
    q = np.arange(GROUP_CH)[:, None]
    m = np.arange(half)[None, :]
    chan = np.zeros((GROUP_CH, GROUP_CH))
    chan[:, :half] = np.cos(2 * np.pi * (q * m % GROUP_CH) / GROUP_CH)
    chan[:, half:] = -np.sin(2 * np.pi * (q * m % GROUP_CH) / GROUP_CH)
    chan[:, half] = np.cos(np.pi * q[:, 0])
    t = np.arange(tok_count)[None, :]
    b = np.arange(tok_count)[:, None]
    scale = 1.0 / math.sqrt(length * GROUP_CH)
    mid = np.zeros((peers, tok_count, 2, tok_count))
    for a in range(peers):
        angle = 2 * np.pi * (t * (peers * b + a) % length) / length
        mid[a, :, 0] = np.cos(angle) * scale
        mid[a, :, 1] = -np.sin(angle) * scale * (1 if a <= peers // 2 else -1)
    mid = mid.reshape(peers, tok_count, 2 * tok_count)[row_slots(peers)]
    fold = np.zeros((GROUP_CH, GROUP_CH))
    fold[0, 0] = 1
    fold[half, half] = 1
    for a in range(1, half):
        fold[a, a] = 1
        fold[a, GROUP_CH - a] = 1
        fold[half + a, a] = 1
        fold[half + a, GROUP_CH - a] = -1
    return [jnp.asarray(x, jnp.bfloat16) for x in (np.stack([chan, fold]), mid)]


def plus(a, b):
    if a is None or b is None:
        return b if a is None else a
    return a + b


def minus(a, b):
    if a is None or b is None:
        return a if b is None else -b
    return a - b


def times(a, factor):
    return None if a is None else a * factor


def widen(a):
    return None if a is None else a.astype(jnp.float32)


def even_transform(x):
    r = math.sqrt(0.5)
    e = [widen(plus(x[s], x[s + 8])) for s in range(8)]
    p04, n04 = plus(e[0], e[4]), minus(e[0], e[4])
    p26, n26 = plus(e[2], e[6]), minus(e[2], e[6])
    p15, n15 = plus(e[1], e[5]), minus(e[1], e[5])
    p37, n37 = plus(e[3], e[7]), minus(e[3], e[7])
    low, high = plus(p04, p26), plus(p15, p37)
    even_cos = times(minus(n15, n37), r)
    even_sin = times(plus(n15, n37), r)
    return {
        0: (plus(low, high), None),
        8: (minus(low, high), None),
        4: (minus(p04, p26), minus(p15, p37)),
        2: (plus(n04, even_cos), plus(even_sin, n26)),
        6: (minus(n04, even_cos), minus(even_sin, n26)),
    }


def odd_transform(x):
    r = math.sqrt(0.5)
    c1, s1 = math.cos(math.pi / 8), math.sin(math.pi / 8)
    o = [widen(minus(x[s], x[s + 8])) for s in range(8)]
    f1, f2, f3 = minus(o[1], o[7]), times(minus(o[2], o[6]), r), minus(o[3], o[5])
    g1, g2, g3 = plus(o[1], o[7]), times(plus(o[2], o[6]), r), plus(o[3], o[5])
    up, down = plus(o[0], f2), minus(o[0], f2)
    one = plus(times(f1, c1), times(f3, s1))
    two = minus(times(f1, s1), times(f3, c1))
    add, sub = plus(g2, o[4]), minus(g2, o[4])
    three = plus(times(g1, s1), times(g3, c1))
    four = minus(times(g1, c1), times(g3, s1))
    return {
        1: (plus(up, one), plus(three, add)),
        7: (minus(up, one), minus(three, add)),
        3: (plus(down, two), plus(four, sub)),
        5: (minus(down, two), minus(four, sub)),
    }


def fused_kernel(
    shape,
    tokens_hbm,
    gain_hbm,
    w_in_hbm,
    small_hbm,
    mid_hbm,
    w_out_hbm,
    last_ref,
    partial_ref,
    w_last,
    tokens,
    gain,
    w_in,
    small,
    mid,
    w_out,
    w_first,
    natural,
    first_out,
    first_in,
    blocks,
    second_out,
    second_in,
    early,
    load_sem,
    send_sem,
    recv_a,
    recv_b,
):
    row_count, col_count = shape
    peers = row_count * col_count
    tok_count, width = tokens.shape
    feat_count = w_in.shape[1]
    fine = tok_count // peers
    groups = feat_count // GROUP_CH
    half = GROUP_CH // 2
    hosts = [r * col_count + c for r, c in host_spots(row_count)]
    row, col = lax.axis_index("row"), lax.axis_index("col")
    me = row * col_count + col
    is_host = me == hosts[0]
    group = jnp.int32(0)
    for g in range(1, groups):
        is_host = is_host | (me == hosts[g])
        group = group + jnp.where(me == hosts[g], g, 0)

    def device(index):
        return {"row": index // col_count, "col": index % col_count}

    load_tokens = pltpu.make_async_copy(tokens_hbm, tokens, load_sem.at[0])
    load_gain = pltpu.make_async_copy(gain_hbm, gain, load_sem.at[1])
    load_small = pltpu.make_async_copy(small_hbm, small, load_sem.at[2])
    load_mid = pltpu.make_async_copy(mid_hbm, mid, load_sem.at[3])
    load_out = pltpu.make_async_copy(w_out_hbm, w_out, load_sem.at[4])
    edges = [sum(CHUNKS[:c]) for c in range(len(CHUNKS) + 1)]
    spans = [
        (edges[c] * GROUP_CH, (edges[c + 1] - edges[c]) * GROUP_CH) for c in range(len(CHUNKS))
    ]
    load_w = []
    for c, (left, size) in enumerate(spans):
        at = (slice(None), pl.ds(left, size))
        load_w.append(pltpu.make_async_copy(w_in_hbm.at[at], w_in.at[at], load_sem.at[5 + c]))
    load_tokens.start()
    load_gain.start()
    load_w[0].start()
    load_small.start()
    for load in load_w[1:]:
        load.start()

    barrier = pltpu.get_barrier_semaphore()

    @pl.when(is_host)
    def _():
        for step in range(1, peers):
            target = lax.rem(me + step, peers)
            pl.semaphore_signal(
                barrier,
                inc=1,
                device_id={"row": target // col_count, "col": lax.rem(target, col_count)},
                device_id_type=MESH,
            )

    load_tokens.wait()
    load_gain.wait()
    scaled = tokens[...] * gain[...].reshape(1, width)
    widened = tokens[...].astype(jnp.float32)
    factor = lax.rsqrt(jnp.mean(widened * widened, -1, keepdims=True) + NORM_EPS)
    for c, (left, size) in enumerate(spans):
        load_w[c].wait()
        if c == len(spans) - 1:

            @pl.when(is_host)
            def _():
                load_mid.start()

            load_out.start()
        mixin = jnp.dot(
            scaled, w_in[:, left : left + size], preferred_element_type=jnp.float32
        )
        mixin = (mixin * factor).astype(jnp.bfloat16)
        if c == 0:
            load_small.wait()
        for g in range(edges[c], edges[c + 1]):
            at = g * GROUP_CH - left
            first_out[g] = jnp.dot(
                mixin[:, at : at + GROUP_CH], small[0], preferred_element_type=jnp.float32
            ).astype(jnp.bfloat16)
        if c == 0:

            @pl.when(is_host)
            def _():
                pl.semaphore_wait(barrier, groups - 1)

            @pl.when(jnp.logical_not(is_host))
            def _():
                pl.semaphore_wait(barrier, groups)

        for g in range(edges[c], edges[c + 1]):
            spot = hosts[g]

            @pl.when(me != spot)
            def _():
                pltpu.make_async_remote_copy(
                    src_ref=first_out.at[g],
                    dst_ref=first_in.at[me],
                    send_sem=send_sem.at[0],
                    recv_sem=recv_a.at[jnp.where(row == row_count - 1, 1, 0)],
                    device_id=device(spot),
                    device_id_type=MESH,
                ).start()

            @pl.when(me == spot)
            def _():
                first_in[me] = first_out[g]

    load_out.wait()
    for g in range(groups):
        span = slice(g * GROUP_CH, (g + 1) * GROUP_CH)
        folded = jnp.dot(small[1], w_out[span, :], preferred_element_type=jnp.float32)
        if g < groups - LATE:
            w_first[span, :] = folded.astype(jnp.bfloat16)
        else:
            at = (g - groups + LATE) * GROUP_CH
            w_last[at : at + GROUP_CH, :] = folded.astype(jnp.bfloat16)

    slots = row_slots(peers)

    @pl.when(is_host)
    def _():
        load_mid.wait()
        step = 16
        late_count = col_count
        late_top = peers - late_count
        rest = first_in.at[pl.ds(0, late_top - 1)]
        pltpu.make_async_copy(rest, rest, recv_a.at[0]).wait()
        for transform in (even_transform, odd_transform):
            for top in range(0, tok_count, step):
                rows = slice(top, top + step)
                arrived = [first_in[s, rows] for s in range(late_top)] + [None] * late_count
                for a, (cosine, sine) in transform(arrived).items():
                    early[a, 0, rows] = cosine
                    if sine is not None:
                        early[a, 1, rows] = sine
        rest = first_in.at[pl.ds(0, late_count)]
        pltpu.make_async_copy(rest, rest, recv_a.at[1]).wait()
        cosine_lane = lax.broadcasted_iota(jnp.int16, (step, LANES), 1) <= half
        zero = jnp.zeros((step, LANES), jnp.bfloat16)
        for parity, transform in enumerate((even_transform, odd_transform)):
            for top in range(0, tok_count, step):
                rows = slice(top, top + step)
                arrived = [None] * late_top + [first_in[s, rows] for s in range(late_top, peers)]
                for a, (cosine, sine) in transform(arrived).items():
                    cosine = plus(early[a, 0, rows], cosine)
                    sine = None if sine is None else plus(early[a, 1, rows], sine)
                    cosine = cosine.astype(jnp.bfloat16)
                    sine = zero if sine is None else sine.astype(jnp.bfloat16)
                    blocks[a, top : top + step] = jnp.where(cosine_lane, cosine, sine)
                    blocks[a, tok_count + top : tok_count + top + step] = jnp.where(
                        cosine_lane, sine, -cosine
                    )
            cuts = (0, peers) if parity == 0 else (0, col_count // 2, peers)
            for first, stop in zip(cuts, cuts[1:]):
                for i in range(parity * peers // 2, (parity + 1) * peers // 2, 2):
                    pair = [
                        jnp.dot(
                            mid[i + n, first * fine : stop * fine],
                            blocks[min(a, peers - a)],
                            preferred_element_type=jnp.float32,
                        ).reshape(stop - first, fine, LANES)
                        for n, a in enumerate(slots[i : i + 2])
                    ]
                    second_out[first:stop, i * fine : (i + 2) * fine, :] = jnp.concatenate(
                        pair, axis=1
                    ).astype(jnp.bfloat16)
                if stop == col_count // 2:
                    for target in range(col_count // 2):
                        pltpu.make_async_remote_copy(
                            src_ref=second_out.at[target],
                            dst_ref=second_in.at[group],
                            send_sem=send_sem.at[1],
                            recv_sem=recv_b.at[group // LATE],
                            device_id=device(target),
                            device_id_type=MESH,
                        ).start()

    served = [0, row_count - 1, *range(1, row_count - 1)]
    served = [r * col_count + c for r in served for c in range(col_count)][col_count // 2 :]
    for g, spot in enumerate(hosts):

        @pl.when(me == spot)
        def _():
            for target in served:
                if target != spot:
                    pltpu.make_async_remote_copy(
                        src_ref=second_out.at[target],
                        dst_ref=second_in.at[g],
                        send_sem=send_sem.at[1],
                        recv_sem=recv_b.at[g // LATE],
                        device_id=device(target),
                        device_id_type=MESH,
                    ).start()
            second_in[g] = second_out[spot]

    @pl.when(is_host)
    def _():
        sent = first_out.at[pl.ds(0, groups - 1)]
        pltpu.make_async_copy(sent, sent, send_sem.at[0]).wait()

    @pl.when(jnp.logical_not(is_host))
    def _():
        pltpu.make_async_copy(first_out, first_out, send_sem.at[0]).wait()

    flipped = jnp.where(lax.broadcasted_iota(jnp.int32, (fine, LANES), 1) > half, -1.0, 1.0)

    def arrive(pair):
        own = (me == hosts[pair * LATE]) | (me == hosts[pair * LATE + 1])

        @pl.when(own)
        def _():
            one = second_in.at[pair * LATE]
            pltpu.make_async_copy(one, one, recv_b.at[pair]).wait()

        @pl.when(jnp.logical_not(own))
        def _():
            both = second_in.at[pl.ds(pair * LATE, LATE)]
            pltpu.make_async_copy(both, both, recv_b.at[pair]).wait()

    def collect(g):
        for i, a in enumerate(slots):
            part = second_in[g, i * fine : (i + 1) * fine].astype(jnp.float32)
            if a > peers // 2:
                part = part * flipped
            natural[g, pl.ds(a, fine, stride=peers), :] = part
        return natural[g].astype(jnp.bfloat16)

    arrive(0)
    values = [collect(g) for g in range(LATE)]
    partial_ref[...] = jnp.dot(
        jnp.concatenate(values, axis=1), w_first[...], preferred_element_type=jnp.float32
    )
    arrive(1)
    for g in range(LATE):
        last_ref[:, g * GROUP_CH : (g + 1) * GROUP_CH] = collect(LATE + g)

    @pl.when(is_host)
    def _():
        sent = second_out.at[pl.ds(0, peers - 1)]
        pltpu.make_async_copy(sent, sent, send_sem.at[1]).wait()


def project_kernel(chunks, last, partial, w_last, out_hbm, staged, sem):
    size = w_last.shape[1] // chunks
    for i in range(chunks):
        lanes = slice(i * size, (i + 1) * size)
        staged[:, lanes] = (
            partial[:, lanes]
            + jnp.dot(last[...], w_last[:, lanes], preferred_element_type=jnp.float32)
        ).astype(staged.dtype)
        span = pl.ds(i * size, size)
        pltpu.make_async_copy(staged.at[:, span], out_hbm.at[:, span], sem).start()
    pltpu.make_async_copy(staged, out_hbm, sem).wait()


def fused_shards(tokens, norm_gain, w_in, w_out):
    seq_count, tok_count, width = tokens.shape
    feat_count = w_in.shape[1]
    shape = (lax.axis_size("row"), lax.axis_size("col"))
    peers = shape[0] * shape[1]
    groups = feat_count // GROUP_CH
    tables = host_tables(peers, tok_count)
    operands = [tokens.reshape(tok_count, width), norm_gain, w_in, *tables, w_out]
    held = [pltpu.VMEM(x.shape, x.dtype) for x in operands]
    last, partial, w_last = pl.pallas_call(
        functools.partial(fused_kernel, shape),
        out_shape=(
            pltpu.VMEM((tok_count, LATE * GROUP_CH), jnp.bfloat16),
            pltpu.VMEM((tok_count, width), jnp.float32),
            pltpu.VMEM((LATE * GROUP_CH, width), jnp.bfloat16),
        ),
        in_specs=[pl.BlockSpec(memory_space=pltpu.HBM)] * len(operands),
        out_specs=(pl.BlockSpec(memory_space=pltpu.VMEM),) * 3,
        scratch_shapes=held
        + [
            pltpu.VMEM((feat_count - LATE * GROUP_CH, width), jnp.bfloat16),
            pltpu.VMEM((groups, tok_count, GROUP_CH), jnp.float32),
            pltpu.VMEM((groups, tok_count, GROUP_CH), jnp.bfloat16),
            pltpu.VMEM((peers, tok_count, GROUP_CH), jnp.bfloat16),
            pltpu.VMEM((peers // 2 + 1, 2 * tok_count, GROUP_CH), jnp.bfloat16),
            pltpu.VMEM((peers, tok_count, GROUP_CH), jnp.bfloat16),
            pltpu.VMEM((groups, tok_count, GROUP_CH), jnp.bfloat16),
            pltpu.VMEM((peers // 2 + 1, 2, tok_count, GROUP_CH), jnp.float32),
            pltpu.SemaphoreType.DMA((5 + len(CHUNKS),)),
            pltpu.SemaphoreType.DMA((2,)),
            pltpu.SemaphoreType.DMA((2,)),
            pltpu.SemaphoreType.DMA((groups // LATE,)),
        ],
        compiler_params=pltpu.CompilerParams(
            collective_id=0, has_side_effects=True, vmem_limit_bytes=62_000_000
        ),
    )(*operands)
    pieces = max(1, width // 512)
    mixed = pl.pallas_call(
        functools.partial(project_kernel, pieces),
        out_shape=jax.ShapeDtypeStruct((tok_count, width), jnp.bfloat16),
        in_specs=[pl.BlockSpec(memory_space=pltpu.VMEM)] * 3,
        out_specs=pl.BlockSpec(memory_space=pltpu.HBM),
        scratch_shapes=[pltpu.VMEM((tok_count, width), jnp.bfloat16), pltpu.SemaphoreType.DMA],
        compiler_params=pltpu.CompilerParams(vmem_limit_bytes=8 * 1024 * 1024),
    )(last, partial, w_last)
    return mixed.reshape(seq_count, tok_count, width)


def shards(tokens, norm_gain, w_in, w_out):
    seq_count, tok_count, _ = tokens.shape
    shape = (lax.axis_size("row"), lax.axis_size("col"))
    if seq_count == 1 and fused_fits(*shape, tok_count, w_in.shape[1]):
        return fused_shards(tokens, norm_gain, w_in, w_out)
    return factored_shards(tokens, norm_gain, w_in, w_out)


def solution(mesh):
    return jax.shard_map(
        shards,
        mesh=mesh,
        in_specs=(P("grp", ("row", "col"), None), P(), P(), P()),
        out_specs=P("grp", ("row", "col"), None),
        check_vma=False,
    )
```

```python
import functools
import math

import jax
import jax.numpy as jnp
import numpy as np
from jax import lax
from jax.experimental import pallas as pl
from jax.experimental.pallas import tpu as pltpu
from jax.sharding import PartitionSpec as P

GROUP_CH = 128


TWO_PI = 2.0 * math.pi
NORM_EPS = 1e-06
HIGHEST = lax.Precision.HIGHEST


def phase_tables(rows, cols, period):
    left = lax.broadcasted_iota(jnp.int32, (rows, cols), 0)
    right = lax.broadcasted_iota(jnp.int32, (rows, cols), 1)
    angles = (left * right % period).astype(jnp.float32) * (TWO_PI / period)
    return (jnp.cos(angles), jnp.sin(angles))


def rotate_by(pattern, cos_table, sin_table, real_part, imag_part):

    def apply(table, data):
        return jnp.einsum(pattern, table, data, precision=HIGHEST)

    return (
        apply(cos_table, real_part) + apply(sin_table, imag_part),
        apply(cos_table, imag_part) - apply(sin_table, real_part),
    )


def twist(real_part, imag_part, cos_table, sin_table):
    return (
        real_part * cos_table + imag_part * sin_table,
        imag_part * cos_table - real_part * sin_table,
    )


def factored_shards(tokens, norm_gain, w_in, w_out):
    seq_count, tok_count, width = tokens.shape
    feat_count = w_in.shape[1]
    row_count = lax.axis_size("row")
    col_count = lax.axis_size("col")
    block_len = tok_count * col_count
    length = block_len * row_count
    sub_feats = feat_count // row_count
    fine_count = tok_count // row_count
    item_count = seq_count * feat_count // col_count
    ortho_scale = 1.0 / math.sqrt(length * GROUP_CH)
    widened = tokens.astype(jnp.float32)
    factor = lax.rsqrt(jnp.mean(widened * widened, -1, keepdims=True) + NORM_EPS)
    normed = (widened * factor * norm_gain.astype(jnp.float32)).astype(jnp.bfloat16)
    mixin = jnp.einsum("std,df->sft", normed, w_in, preferred_element_type=jnp.float32).astype(
        jnp.bfloat16
    )
    row_cos, row_sin = phase_tables(row_count, row_count, row_count)
    chan_cos, chan_sin = phase_tables(GROUP_CH, GROUP_CH, GROUP_CH)
    stacked_shape = (seq_count, sub_feats, row_count, tok_count)
    grouped = mixin.astype(jnp.float32).reshape(
        seq_count, feat_count // GROUP_CH, GROUP_CH, tok_count
    )
    spec_real = jnp.einsum("sgqt,qm->sgmt", grouped, chan_cos, precision=HIGHEST).reshape(
        seq_count, feat_count, tok_count
    )
    spec_imag = -jnp.einsum("sgqt,qm->sgmt", grouped, chan_sin, precision=HIGHEST).reshape(
        seq_count, feat_count, tok_count
    )
    arrived = (
        lax.all_to_all(
            spec_real.astype(jnp.bfloat16), "row", split_axis=1, concat_axis=2, tiled=True
        ).astype(spec_real.dtype),
        lax.all_to_all(
            spec_imag.astype(jnp.bfloat16), "row", split_axis=1, concat_axis=2, tiled=True
        ).astype(spec_imag.dtype),
    )
    stacked_real = arrived[0].reshape(stacked_shape)
    stacked_imag = arrived[1].reshape(stacked_shape)
    real_part, imag_part = rotate_by("ka,sfat->skft", row_cos, row_sin, stacked_real, stacked_imag)
    freq_low = lax.broadcasted_iota(jnp.int32, (row_count, tok_count), 0)
    place = lax.axis_index("col") * tok_count + lax.broadcasted_iota(
        jnp.int32, (row_count, tok_count), 1
    )
    angles = (freq_low * place % length).astype(jnp.float32) * (TWO_PI / length)
    real_part, imag_part = twist(
        real_part, imag_part, jnp.cos(angles)[None, :, None, :], jnp.sin(angles)[None, :, None, :]
    )
    sending = (
        real_part.reshape(item_count, col_count, 1, tok_count),
        imag_part.reshape(item_count, col_count, 1, tok_count),
    )
    col_cos, col_sin = phase_tables(col_count, col_count, col_count)
    mid_cos, mid_sin = phase_tables(col_count, tok_count, block_len)
    tok_cos, tok_sin = phase_tables(tok_count, tok_count, tok_count)
    tok_cos = tok_cos.reshape(row_count, fine_count, tok_count)
    tok_sin = tok_sin.reshape(row_count, fine_count, tok_count)
    span_real, span_imag = rotate_by(
        "uc,qct->qut",
        col_cos,
        col_sin,
        lax.all_to_all(
            sending[0].astype(jnp.bfloat16), "col", split_axis=1, concat_axis=2, tiled=True
        ).astype(jnp.float32)[:, 0],
        lax.all_to_all(
            sending[1].astype(jnp.bfloat16), "col", split_axis=1, concat_axis=2, tiled=True
        ).astype(jnp.float32)[:, 0],
    )
    span_real, span_imag = twist(span_real, span_imag, mid_cos, mid_sin)
    span_real, span_imag = rotate_by("rjt,qut->rjuq", tok_cos, tok_sin, span_real, span_imag)
    owner_shape = (row_count, col_count, fine_count, span_real.shape[-1], 1)
    span_real, span_imag = (span_real.reshape(owner_shape), span_imag.reshape(owner_shape))
    rounded = (span_real * ortho_scale).astype(jnp.bfloat16)
    returned = lax.all_to_all(rounded, "col", split_axis=1, concat_axis=4, tiled=True)
    layout = (row_count, fine_count, seq_count, row_count, sub_feats)
    spectrum = lax.all_to_all(
        returned.reshape(layout), "row", split_axis=0, concat_axis=4, tiled=True
    )
    spectrum = spectrum.reshape(fine_count, seq_count, row_count, feat_count)
    mixed = jnp.einsum("jskf,fd->sjkd", spectrum, w_out, preferred_element_type=jnp.float32).astype(
        jnp.bfloat16
    )
    return mixed.reshape(seq_count, fine_count * row_count, width)


CHUNKS = (1, 3)
LATE = 2
LANES = 128
MESH = pl.DeviceIdType.MESH


def host_spots(row_count):
    low, high = row_count // 2 - 1, row_count // 2
    return [(low, 1), (low, 3), (high, 3), (high, 1)]


def fused_fits(row_count, col_count, tok_count, feat_count):
    return (
        row_count == 4
        and col_count == 4
        and tok_count == LANES
        and GROUP_CH == LANES
        and feat_count == GROUP_CH * 4
    )


def row_slots(peers):
    pairs = [(0, peers // 2)] + [(a, peers - a) for a in range(1, peers // 2)]
    return [a for parity in (0, 1) for pair in pairs if pair[0] % 2 == parity for a in pair]


def host_tables(peers, tok_count):
    length = peers * tok_count
    half = GROUP_CH // 2
    q = np.arange(GROUP_CH)[:, None]
    m = np.arange(half)[None, :]
    chan = np.zeros((GROUP_CH, GROUP_CH))
    chan[:, :half] = np.cos(2 * np.pi * (q * m % GROUP_CH) / GROUP_CH)
    chan[:, half:] = -np.sin(2 * np.pi * (q * m % GROUP_CH) / GROUP_CH)
    chan[:, half] = np.cos(np.pi * q[:, 0])
    t = np.arange(tok_count)[None, :]
    b = np.arange(tok_count)[:, None]
    scale = 1.0 / math.sqrt(length * GROUP_CH)
    mid = np.zeros((peers, tok_count, 2, tok_count))
    for a in range(peers):
        angle = 2 * np.pi * (t * (peers * b + a) % length) / length
        mid[a, :, 0] = np.cos(angle) * scale
        mid[a, :, 1] = -np.sin(angle) * scale * (1 if a <= peers // 2 else -1)
    mid = mid.reshape(peers, tok_count, 2 * tok_count)[row_slots(peers)]
    fold = np.zeros((GROUP_CH, GROUP_CH))
    fold[0, 0] = 1
    fold[half, half] = 1
    for a in range(1, half):
        fold[a, a] = 1
        fold[a, GROUP_CH - a] = 1
        fold[half + a, a] = 1
        fold[half + a, GROUP_CH - a] = -1
    return [jnp.asarray(x, jnp.bfloat16) for x in (np.stack([chan, fold]), mid)]


def plus(a, b):
    if a is None or b is None:
        return b if a is None else a
    return a + b


def minus(a, b):
    if a is None or b is None:
        return a if b is None else -b
    return a - b


def times(a, factor):
    return None if a is None else a * factor


def widen(a):
    return None if a is None else a.astype(jnp.float32)


def even_transform(x):
    r = math.sqrt(0.5)
    e = [widen(plus(x[s], x[s + 8])) for s in range(8)]
    p04, n04 = plus(e[0], e[4]), minus(e[0], e[4])
    p26, n26 = plus(e[2], e[6]), minus(e[2], e[6])
    p15, n15 = plus(e[1], e[5]), minus(e[1], e[5])
    p37, n37 = plus(e[3], e[7]), minus(e[3], e[7])
    low, high = plus(p04, p26), plus(p15, p37)
    even_cos = times(minus(n15, n37), r)
    even_sin = times(plus(n15, n37), r)
    return {
        0: (plus(low, high), None),
        8: (minus(low, high), None),
        4: (minus(p04, p26), minus(p15, p37)),
        2: (plus(n04, even_cos), plus(even_sin, n26)),
        6: (minus(n04, even_cos), minus(even_sin, n26)),
    }


def odd_transform(x):
    r = math.sqrt(0.5)
    c1, s1 = math.cos(math.pi / 8), math.sin(math.pi / 8)
    o = [widen(minus(x[s], x[s + 8])) for s in range(8)]
    f1, f2, f3 = minus(o[1], o[7]), times(minus(o[2], o[6]), r), minus(o[3], o[5])
    g1, g2, g3 = plus(o[1], o[7]), times(plus(o[2], o[6]), r), plus(o[3], o[5])
    up, down = plus(o[0], f2), minus(o[0], f2)
    one = plus(times(f1, c1), times(f3, s1))
    two = minus(times(f1, s1), times(f3, c1))
    add, sub = plus(g2, o[4]), minus(g2, o[4])
    three = plus(times(g1, s1), times(g3, c1))
    four = minus(times(g1, c1), times(g3, s1))
    return {
        1: (plus(up, one), plus(three, add)),
        7: (minus(up, one), minus(three, add)),
        3: (plus(down, two), plus(four, sub)),
        5: (minus(down, two), minus(four, sub)),
    }


def fused_kernel(
    shape,
    tokens_hbm,
    gain_hbm,
    w_in_hbm,
    small_hbm,
    mid_hbm,
    w_out_hbm,
    last_ref,
    partial_ref,
    w_last,
    tokens,
    gain,
    w_in,
    small,
    mid,
    w_out,
    w_first,
    natural,
    first_out,
    first_in,
    blocks,
    second_out,
    second_in,
    early,
    load_sem,
    send_sem,
    recv_a,
    recv_b,
):
    row_count, col_count = shape
    peers = row_count * col_count
    tok_count, width = tokens.shape
    feat_count = w_in.shape[1]
    fine = tok_count // peers
    groups = feat_count // GROUP_CH
    half = GROUP_CH // 2
    hosts = [r * col_count + c for r, c in host_spots(row_count)]
    row, col = lax.axis_index("row"), lax.axis_index("col")
    me = row * col_count + col
    is_host = me == hosts[0]
    group = jnp.int32(0)
    for g in range(1, groups):
        is_host = is_host | (me == hosts[g])
        group = group + jnp.where(me == hosts[g], g, 0)

    def device(index):
        return {"row": index // col_count, "col": index % col_count}

    load_tokens = pltpu.make_async_copy(tokens_hbm, tokens, load_sem.at[0])
    load_gain = pltpu.make_async_copy(gain_hbm, gain, load_sem.at[1])
    load_small = pltpu.make_async_copy(small_hbm, small, load_sem.at[2])
    load_mid = pltpu.make_async_copy(mid_hbm, mid, load_sem.at[3])
    load_out = pltpu.make_async_copy(w_out_hbm, w_out, load_sem.at[4])
    edges = [sum(CHUNKS[:c]) for c in range(len(CHUNKS) + 1)]
    spans = [
        (edges[c] * GROUP_CH, (edges[c + 1] - edges[c]) * GROUP_CH) for c in range(len(CHUNKS))
    ]
    load_w = []
    for c, (left, size) in enumerate(spans):
        at = (slice(None), pl.ds(left, size))
        load_w.append(pltpu.make_async_copy(w_in_hbm.at[at], w_in.at[at], load_sem.at[5 + c]))
    load_tokens.start()
    load_gain.start()
    load_w[0].start()
    load_small.start()
    for load in load_w[1:]:
        load.start()

    barrier = pltpu.get_barrier_semaphore()

    @pl.when(is_host)
    def _():
        for step in range(1, peers):
            target = lax.rem(me + step, peers)
            pl.semaphore_signal(
                barrier,
                inc=1,
                device_id={"row": target // col_count, "col": lax.rem(target, col_count)},
                device_id_type=MESH,
            )

    load_tokens.wait()
    load_gain.wait()
    scaled = tokens[...] * gain[...].reshape(1, width)
    widened = tokens[...].astype(jnp.float32)
    factor = lax.rsqrt(jnp.mean(widened * widened, -1, keepdims=True) + NORM_EPS)
    for c, (left, size) in enumerate(spans):
        load_w[c].wait()
        if c == len(spans) - 1:

            @pl.when(is_host)
            def _():
                load_mid.start()

            load_out.start()
        mixin = jnp.dot(
            scaled, w_in[:, left : left + size], preferred_element_type=jnp.float32
        )
        mixin = (mixin * factor).astype(jnp.bfloat16)
        if c == 0:
            load_small.wait()
        for g in range(edges[c], edges[c + 1]):
            at = g * GROUP_CH - left
            first_out[g] = jnp.dot(
                mixin[:, at : at + GROUP_CH], small[0], preferred_element_type=jnp.float32
            ).astype(jnp.bfloat16)
        if c == 0:

            @pl.when(is_host)
            def _():
                pl.semaphore_wait(barrier, groups - 1)

            @pl.when(jnp.logical_not(is_host))
            def _():
                pl.semaphore_wait(barrier, groups)

        for g in range(edges[c], edges[c + 1]):
            spot = hosts[g]

            @pl.when(me != spot)
            def _():
                pltpu.make_async_remote_copy(
                    src_ref=first_out.at[g],
                    dst_ref=first_in.at[me],
                    send_sem=send_sem.at[0],
                    recv_sem=recv_a.at[jnp.where(row == row_count - 1, 1, 0)],
                    device_id=device(spot),
                    device_id_type=MESH,
                ).start()

            @pl.when(me == spot)
            def _():
                first_in[me] = first_out[g]

    load_out.wait()
    for g in range(groups):
        span = slice(g * GROUP_CH, (g + 1) * GROUP_CH)
        folded = jnp.dot(small[1], w_out[span, :], preferred_element_type=jnp.float32)
        if g < groups - LATE:
            w_first[span, :] = folded.astype(jnp.bfloat16)
        else:
            at = (g - groups + LATE) * GROUP_CH
            w_last[at : at + GROUP_CH, :] = folded.astype(jnp.bfloat16)

    slots = row_slots(peers)

    @pl.when(is_host)
    def _():
        load_mid.wait()
        step = 16
        late_count = col_count
        late_top = peers - late_count
        rest = first_in.at[pl.ds(0, late_top - 1)]
        pltpu.make_async_copy(rest, rest, recv_a.at[0]).wait()
        for transform in (even_transform, odd_transform):
            for top in range(0, tok_count, step):
                rows = slice(top, top + step)
                arrived = [first_in[s, rows] for s in range(late_top)] + [None] * late_count
                for a, (cosine, sine) in transform(arrived).items():
                    early[a, 0, rows] = cosine
                    if sine is not None:
                        early[a, 1, rows] = sine
        rest = first_in.at[pl.ds(0, late_count)]
        pltpu.make_async_copy(rest, rest, recv_a.at[1]).wait()
        cosine_lane = lax.broadcasted_iota(jnp.int16, (step, LANES), 1) <= half
        zero = jnp.zeros((step, LANES), jnp.bfloat16)
        for parity, transform in enumerate((even_transform, odd_transform)):
            for top in range(0, tok_count, step):
                rows = slice(top, top + step)
                arrived = [None] * late_top + [first_in[s, rows] for s in range(late_top, peers)]
                for a, (cosine, sine) in transform(arrived).items():
                    cosine = plus(early[a, 0, rows], cosine)
                    sine = None if sine is None else plus(early[a, 1, rows], sine)
                    cosine = cosine.astype(jnp.bfloat16)
                    sine = zero if sine is None else sine.astype(jnp.bfloat16)
                    blocks[a, top : top + step] = jnp.where(cosine_lane, cosine, sine)
                    blocks[a, tok_count + top : tok_count + top + step] = jnp.where(
                        cosine_lane, sine, -cosine
                    )
            cuts = (0, peers) if parity == 0 else (0, col_count, peers)
            for first, stop in zip(cuts, cuts[1:]):
                for i in range(parity * peers // 2, (parity + 1) * peers // 2, 2):
                    pair = [
                        jnp.dot(
                            mid[i + n, first * fine : stop * fine],
                            blocks[min(a, peers - a)],
                            preferred_element_type=jnp.float32,
                        ).reshape(stop - first, fine, LANES)
                        for n, a in enumerate(slots[i : i + 2])
                    ]
                    second_out[first:stop, i * fine : (i + 2) * fine, :] = jnp.concatenate(
                        pair, axis=1
                    ).astype(jnp.bfloat16)
                if stop == col_count:
                    for target in range(col_count):
                        pltpu.make_async_remote_copy(
                            src_ref=second_out.at[target],
                            dst_ref=second_in.at[group],
                            send_sem=send_sem.at[1],
                            recv_sem=recv_b.at[group // LATE],
                            device_id=device(target),
                            device_id_type=MESH,
                        ).start()

    served = [row_count - 1, *range(1, row_count - 1)]
    served = [r * col_count + c for r in served for c in range(col_count)]
    for g, spot in enumerate(hosts):

        @pl.when(me == spot)
        def _():
            for target in served:
                if target != spot:
                    pltpu.make_async_remote_copy(
                        src_ref=second_out.at[target],
                        dst_ref=second_in.at[g],
                        send_sem=send_sem.at[1],
                        recv_sem=recv_b.at[g // LATE],
                        device_id=device(target),
                        device_id_type=MESH,
                    ).start()
            second_in[g] = second_out[spot]

    @pl.when(is_host)
    def _():
        sent = first_out.at[pl.ds(0, groups - 1)]
        pltpu.make_async_copy(sent, sent, send_sem.at[0]).wait()

    @pl.when(jnp.logical_not(is_host))
    def _():
        pltpu.make_async_copy(first_out, first_out, send_sem.at[0]).wait()

    flipped = jnp.where(lax.broadcasted_iota(jnp.int32, (fine, LANES), 1) > half, -1.0, 1.0)

    def arrive(pair):
        own = (me == hosts[pair * LATE]) | (me == hosts[pair * LATE + 1])

        @pl.when(own)
        def _():
            one = second_in.at[pair * LATE]
            pltpu.make_async_copy(one, one, recv_b.at[pair]).wait()

        @pl.when(jnp.logical_not(own))
        def _():
            both = second_in.at[pl.ds(pair * LATE, LATE)]
            pltpu.make_async_copy(both, both, recv_b.at[pair]).wait()

    def collect(g):
        for i, a in enumerate(slots):
            part = second_in[g, i * fine : (i + 1) * fine].astype(jnp.float32)
            if a > peers // 2:
                part = part * flipped
            natural[g, pl.ds(a, fine, stride=peers), :] = part
        return natural[g].astype(jnp.bfloat16)

    arrive(0)
    values = [collect(g) for g in range(LATE)]
    partial_ref[...] = jnp.dot(
        jnp.concatenate(values, axis=1), w_first[...], preferred_element_type=jnp.float32
    )
    arrive(1)
    for g in range(LATE):
        last_ref[:, g * GROUP_CH : (g + 1) * GROUP_CH] = collect(LATE + g)

    @pl.when(is_host)
    def _():
        sent = second_out.at[pl.ds(0, peers - 1)]
        pltpu.make_async_copy(sent, sent, send_sem.at[1]).wait()


def project_kernel(chunks, last, partial, w_last, out_hbm, staged, sem):
    size = w_last.shape[1] // chunks
    for i in range(chunks):
        lanes = slice(i * size, (i + 1) * size)
        staged[:, lanes] = (
            partial[:, lanes]
            + jnp.dot(last[...], w_last[:, lanes], preferred_element_type=jnp.float32)
        ).astype(staged.dtype)
        span = pl.ds(i * size, size)
        pltpu.make_async_copy(staged.at[:, span], out_hbm.at[:, span], sem).start()
    pltpu.make_async_copy(staged, out_hbm, sem).wait()


def fused_shards(tokens, norm_gain, w_in, w_out):
    seq_count, tok_count, width = tokens.shape
    feat_count = w_in.shape[1]
    shape = (lax.axis_size("row"), lax.axis_size("col"))
    peers = shape[0] * shape[1]
    groups = feat_count // GROUP_CH
    tables = host_tables(peers, tok_count)
    operands = [tokens.reshape(tok_count, width), norm_gain, w_in, *tables, w_out]
    held = [pltpu.VMEM(x.shape, x.dtype) for x in operands]
    last, partial, w_last = pl.pallas_call(
        functools.partial(fused_kernel, shape),
        out_shape=(
            pltpu.VMEM((tok_count, LATE * GROUP_CH), jnp.bfloat16),
            pltpu.VMEM((tok_count, width), jnp.float32),
            pltpu.VMEM((LATE * GROUP_CH, width), jnp.bfloat16),
        ),
        in_specs=[pl.BlockSpec(memory_space=pltpu.HBM)] * len(operands),
        out_specs=(pl.BlockSpec(memory_space=pltpu.VMEM),) * 3,
        scratch_shapes=held
        + [
            pltpu.VMEM((feat_count - LATE * GROUP_CH, width), jnp.bfloat16),
            pltpu.VMEM((groups, tok_count, GROUP_CH), jnp.float32),
            pltpu.VMEM((groups, tok_count, GROUP_CH), jnp.bfloat16),
            pltpu.VMEM((peers, tok_count, GROUP_CH), jnp.bfloat16),
            pltpu.VMEM((peers // 2 + 1, 2 * tok_count, GROUP_CH), jnp.bfloat16),
            pltpu.VMEM((peers, tok_count, GROUP_CH), jnp.bfloat16),
            pltpu.VMEM((groups, tok_count, GROUP_CH), jnp.bfloat16),
            pltpu.VMEM((peers // 2 + 1, 2, tok_count, GROUP_CH), jnp.float32),
            pltpu.SemaphoreType.DMA((5 + len(CHUNKS),)),
            pltpu.SemaphoreType.DMA((2,)),
            pltpu.SemaphoreType.DMA((2,)),
            pltpu.SemaphoreType.DMA((groups // LATE,)),
        ],
        compiler_params=pltpu.CompilerParams(
            collective_id=0, has_side_effects=True, vmem_limit_bytes=62_000_000
        ),
    )(*operands)
    pieces = max(1, width // 256)
    mixed = pl.pallas_call(
        functools.partial(project_kernel, pieces),
        out_shape=jax.ShapeDtypeStruct((tok_count, width), jnp.bfloat16),
        in_specs=[pl.BlockSpec(memory_space=pltpu.VMEM)] * 3,
        out_specs=pl.BlockSpec(memory_space=pltpu.HBM),
        scratch_shapes=[pltpu.VMEM((tok_count, width), jnp.bfloat16), pltpu.SemaphoreType.DMA],
        compiler_params=pltpu.CompilerParams(vmem_limit_bytes=8 * 1024 * 1024),
    )(last, partial, w_last)
    return mixed.reshape(seq_count, tok_count, width)


def shards(tokens, norm_gain, w_in, w_out):
    seq_count, tok_count, _ = tokens.shape
    shape = (lax.axis_size("row"), lax.axis_size("col"))
    if seq_count == 1 and fused_fits(*shape, tok_count, w_in.shape[1]):
        return fused_shards(tokens, norm_gain, w_in, w_out)
    return factored_shards(tokens, norm_gain, w_in, w_out)


def solution(mesh):
    return jax.shard_map(
        shards,
        mesh=mesh,
        in_specs=(P("grp", ("row", "col"), None), P(), P(), P()),
        out_specs=P("grp", ("row", "col"), None),
        check_vma=False,
    )
```
